512 devices in a mesh: ep: 32 (over z, x), tp: 16 (over y, core).
Axes of the slice: x: 4, y: 8, z: 8, core: 2. Of those that a mesh axis runs over, the one named last changes fastest.
Arguments:
- mixer_group_input: bfloat16 [8192, 1024], P('ep', 'tp'), may hold values from -6 to 6
- log_step_size: float32 [64, 8192], P('tp', 'ep'), may hold values from -16 to 0
- extra_log_decay: float32 [64, 8192], P('tp', 'ep'), may hold values from -0.7 to 0
- negated_eigen_real: float32 [64, 64], P('tp'), may hold values from 0.35 to 0.7
- frequency: float32 [64, 64], P('tp'), may hold values from 0 to 200
- group_input_matrices: bfloat16 [2, 64, 64, 16], P(None, 'tp'), may hold values from -1.5 to 1.5
- group_output_matrices: bfloat16 [2, 64, 16, 64], P(None, 'tp'), may hold values from -0.5 to 0.5
- channel_feedthrough: float32 [1024], P('tp'), may hold values from -3 to 3
- mixer_norm_scale: float32 [1024], replicated, may hold values from 0.1 to 1.9
- mixer_output_weight: bfloat16 [1024, 2048], P(None, 'tp'), may hold values from -0.1875 to 0.1875
- second_micro_input: bfloat16 [4096, 2048], P('ep'), may hold values from -6 to 6
- expert_norm_scale: float32 [2048], replicated, may hold values from 0.1 to 1.9
- routes: int32 [4096, 4], P('ep'), may hold values from 0 to 31, all different within a row; in each aligned block of 128 rows (0 to 127, 128 to 255, ...) at most 32 rows name the same one
- chosen_expert_weight: float32 [4096, 4], P('ep'), may hold values from 0.1 to 1
- expert_gate_weight: bfloat16 [32, 2048, 2048], P('ep', None, 'tp'), may hold values from -0.125 to 0.125
- expert_up_weight: bfloat16 [32, 2048, 2048], P('ep', None, 'tp'), may hold values from -0.125 to 0.125
- expert_down_weight: bfloat16 [32, 2048, 2048], P('ep', None, 'tp'), may hold values from -0.125 to 0.125
- shared_gate_weight: bfloat16 [2048, 2048], P(None, 'tp'), may hold values from -0.125 to 0.125
- shared_up_weight: bfloat16 [2048, 2048], P(None, 'tp'), may hold values from -0.125 to 0.125
- shared_down_weight: bfloat16 [2048, 2048], P(None, 'tp'), may hold values from -0.125 to 0.125
Outputs:
- mixed: bfloat16 [8192, 2048], P('ep', 'tp')
- moe_out: bfloat16 [4096, 2048], P('ep', 'tp')
The draws below stay inside these ranges and needn't reach their ends.
Inputs may be any that keep to these rules, and one draw needn't show every extreme that they name: `routes`: each row names 4 different experts; in each aligned block of 128 rows no expert is named by more than 32 rows, and in some block one expert is named by exactly 32 rows.
All inputs are finite; a program needn't handle non-finite values.
Results may differ from the reference program's by a relative error of at most 0.0068.
Values may be sent and summed in bfloat16 or wider, within the bound.
No kernel may reach another device: no remote copies, remote signals or barrier semaphores. Data moves between devices by JAX's collectives and lax.ppermute only.
A program may use at most 128 MiB of HBM per device.

```python
import math
import jax
import jax.numpy as jnp
import numpy as np
from jax import lax

D = 2048
GROUPS = 64
GROUP_CH = 16
STATE = 64
WIDTH_SSM = 1024
FE = 2048
TOP_K = 4
TOKENS_PER_SHARD = 256
TOK_EP2 = 128
EXPERTS = 32
CAP = 32
TOKENS1 = 8192
TOKENS2 = 4096
N_EP = 32


def draw_log_step_size(key, part):
    base_key = jax.random.fold_in(key, 101)
    slow_key, fast_key, level_key, block_key, rough_key = jax.random.split(base_key, 5)
    slow_share = 0.5
    slow = jax.random.uniform(slow_key, (GROUPS,), jnp.float32) < slow_share
    fast_step = jax.random.uniform(fast_key, (GROUPS,), jnp.float32, 0.045, 0.09)
    slow_step = jax.random.uniform(level_key, (GROUPS,), jnp.float32, 0.15, 0.3) / (0.7 * TOKENS1)
    base = jnp.log(jnp.where(slow, slow_step, fast_step))
    block_count = TOKENS1 // TOKENS_PER_SHARD
    block_factor = jax.random.uniform(block_key, (GROUPS, block_count), jnp.float32, -0.7, 0.7)
    rough = jax.random.uniform(rough_key, (GROUPS, TOKENS1), jnp.float32, -0.4, 0.4)
    return base[:, None] + jnp.repeat(block_factor, TOKENS_PER_SHARD, axis=1) + rough


def draw_extra_log_decay(key, part):
    base_key = jax.random.fold_in(key, 202)
    place_key, size_key = jax.random.split(base_key)
    places = jax.random.randint(place_key, (GROUPS, 2), 0, TOKENS1)
    sizes_log = jnp.log(jax.random.uniform(size_key, (GROUPS, 2), jnp.float32, 0.5, 0.8))
    positions = jnp.arange(TOKENS1, dtype=jnp.int32)
    hits = positions[None, :, None] == places[:, None, :]
    return jnp.sum(jnp.where(hits, sizes_log[:, None, :], 0.0), axis=2)


def block_scale(key, extent, cuts, least, top_value):
    loudness = 1.0
    for dim, blocks in cuts:
        heights = jax.random.uniform(jax.random.fold_in(jax.random.fold_in(key, 6), dim), (blocks,), jnp.float32, least / len(cuts), top_value / len(cuts))
        loudness = loudness * jnp.repeat(jnp.exp(heights), extent[dim] // blocks).reshape((-1,) + (1,) * (len(extent) - 1 - dim))
    return loudness


def shared_out(rng, own, number, rows, count, top, limit, slope):
    ranking = jax.random.permutation(rng, count)
    heavy_load, usual = shares(count, rows * top, limit, slope, True), shares(count, rows * top, limit, slope, False)
    places = jnp.arange(count)

    def named(lengths, turn):
        used = int((lengths > 0).sum())
        fixed = max(1, used // 4)
        shifted = fixed + (places - fixed + turn * (used - fixed)) % max(1, count - fixed)
        return jnp.zeros((count,), jnp.int32).at[ranking[jnp.where(places < fixed, places, shifted)]].set(jnp.asarray(lengths, jnp.int32))

    lengths = jnp.where(number % 4 == 0, named(heavy_load, number // 4), named(usual, number - number // 4 - 1))
    mixed = jax.random.permutation(jax.random.fold_in(own, 3), count)
    donor, sink = mixed[0:count // 2 * 2:2], mixed[1:count // 2 * 2:2]
    room = jnp.minimum(lengths[donor] - 1, limit - lengths[sink]) // 2
    room = jnp.where((donor == ranking[0]) | (sink == ranking[0]) | (lengths[sink] == 0), 0, jnp.maximum(room, 0))
    shifted = jax.random.randint(jax.random.fold_in(own, 4), (count // 2,), 0, 1 << 20) % (room + 1)
    lengths = lengths.at[donor].add(-shifted).at[sink].add(shifted)
    members = jnp.searchsorted(jnp.cumsum(lengths), jnp.arange(rows * top), side="right").astype(jnp.int32)
    listing = members.reshape(top, rows).T
    listing = listing[jax.random.permutation(jax.random.fold_in(own, 1), rows)]
    turn = jax.random.randint(jax.random.fold_in(own, 2), (rows, 1), 0, top)
    return jnp.take_along_axis(listing, (jnp.arange(top)[None, :] + turn) % top, axis=1)


def shares(amount, total, reach, lean, full):
    weights = [(1 << 20) // math.isqrt(rank ** lean) + 1 for rank in range(1, amount + 1)]
    largest = reach if full else min(reach, max(-(-total // amount), total * weights[0] // sum(weights)))
    least = 1 if total - largest >= amount - 1 else 0
    counts, rest = [largest] + [least] * (amount - 1), total - largest - least * (amount - 1)
    while rest > 0:
        free = [i for i in range(1, amount) if counts[i] < largest] or [i for i in range(1, amount) if counts[i] < reach]
        mass, remaining = sum([weights[i] for i in free]), rest
        for i in free:
            more = min(reach - counts[i], max(1, remaining * weights[i] // mass), rest)
            counts[i] = counts[i] + more
            rest = rest - more
    return np.array(counts)


def normal_values(rng, extent, scale, most, cuts=(), held_as=jnp.bfloat16):
    drawn = jax.random.normal(rng, extent, jnp.float32) * scale
    if len(cuts) > 0:
        drawn = block_scale(rng, extent, cuts, -0.22, 0.18) * drawn
    return jnp.clip(drawn, min=-most, max=most).astype(held_as)


def setup_inputs(seed: int = 0) -> dict:
    key_of = jax.random.split(jax.random.key(seed), 21)
    mixer_group_input = normal_values(key_of[0], (TOKENS1, WIDTH_SSM), 1.0, 6.0, ((0, 32), (1, 16)))
    log_step_size = draw_log_step_size(jax.random.fold_in(key_of[20], 71), 0)
    extra_log_decay = draw_extra_log_decay(jax.random.fold_in(key_of[20], 71), 0)
    negated_eigen_real = jnp.clip(jnp.exp(math.log(0.7) - 0.6931472 * jax.random.uniform(key_of[3], (GROUPS, STATE), jnp.float32) ** block_scale(key_of[3], (GROUPS, STATE), ((0, 16),), -0.2, 0.2)), 0.35, 0.7)
    frequency = jnp.clip(200.0 * jax.random.uniform(key_of[4], (GROUPS, STATE), jnp.float32) ** block_scale(key_of[4], (GROUPS, STATE), ((0, 16),), -0.2, 0.2), 0.0, 200.0)
    group_input_matrices = normal_values(key_of[5], (2, GROUPS, STATE, GROUP_CH), GROUP_CH ** -0.5, 1.5, ((1, 16),))
    group_output_matrices = normal_values(key_of[6], (2, GROUPS, GROUP_CH, STATE), (2 * STATE) ** -0.5, 0.5, ((1, 16),))
    channel_feedthrough = normal_values(key_of[7], (WIDTH_SSM,), 0.5, 3.0, ((0, 16),), jnp.float32)
    mixer_norm_scale = jnp.clip(1.0 + 0.18 * jax.random.normal(key_of[8], (WIDTH_SSM,), jnp.float32), 0.1, 1.9)
    mixer_output_weight = normal_values(key_of[9], (WIDTH_SSM, D), WIDTH_SSM ** -0.5, 0.1875, ((1, 16),))
    second_micro_input = normal_values(key_of[10], (TOKENS2, D), 1.0, 6.0, ((0, 32),))
    expert_norm_scale = jnp.clip(1.0 + 0.18 * jax.random.normal(key_of[11], (D,), jnp.float32), 0.1, 1.9)
    routes_keys = jax.random.split(jax.random.fold_in(key_of[12], 1), TOKENS2 // TOK_EP2)
    routes_turns = jax.random.permutation(jax.random.fold_in(key_of[12], 3), TOKENS2 // TOK_EP2)
    routes = jax.vmap(lambda own, number: shared_out(jax.random.fold_in(key_of[12], 2), own, number, TOK_EP2, EXPERTS, TOP_K, CAP, 1))(routes_keys, routes_turns).reshape((TOKENS2, TOP_K))
    chosen_expert_weight = jnp.clip(jnp.exp(math.log(1.0) - 2.3025851 * jax.random.uniform(key_of[13], (TOKENS2, TOP_K), jnp.float32) ** block_scale(key_of[13], (TOKENS2, TOP_K), ((0, 32),), -0.2, 0.2)), 0.1, 1.0)
    expert_gate_weight = normal_values(key_of[14], (EXPERTS, D, FE), D ** -0.5, 0.125, ((0, 32), (2, 16)))
    expert_up_weight = normal_values(key_of[15], (EXPERTS, D, FE), D ** -0.5, 0.125, ((0, 32), (2, 16)))
    expert_down_weight = normal_values(key_of[16], (EXPERTS, FE, D), FE ** -0.5, 0.125, ((0, 32), (2, 16)))
    shared_gate_weight = normal_values(key_of[17], (D, FE), D ** -0.5, 0.125, ((1, 16),))
    shared_up_weight = normal_values(key_of[18], (D, FE), D ** -0.5, 0.125, ((1, 16),))
    shared_down_weight = normal_values(key_of[19], (FE, D), FE ** -0.5, 0.125, ((1, 16),))
    return {"mixer_group_input": mixer_group_input, "log_step_size": log_step_size, "extra_log_decay": extra_log_decay, "negated_eigen_real": negated_eigen_real, "frequency": frequency, "group_input_matrices": group_input_matrices, "group_output_matrices": group_output_matrices, "channel_feedthrough": channel_feedthrough, "mixer_norm_scale": mixer_norm_scale, "mixer_output_weight": mixer_output_weight, "second_micro_input": second_micro_input, "expert_norm_scale": expert_norm_scale, "routes": routes, "chosen_expert_weight": chosen_expert_weight, "expert_gate_weight": expert_gate_weight, "expert_up_weight": expert_up_weight, "expert_down_weight": expert_down_weight, "shared_gate_weight": shared_gate_weight, "shared_up_weight": shared_up_weight, "shared_down_weight": shared_down_weight}


eps_norm = 1e-06

def combine_steps(earlier, latter):
    return (earlier[0] * latter[0] - earlier[1] * latter[1], earlier[0] * latter[1] + earlier[1] * latter[0], latter[0] * earlier[2] - latter[1] * earlier[3] + latter[2], latter[0] * earlier[3] + latter[1] * earlier[2] + latter[3])

def local_states(inputs, step_logs, losses, negated_eigen_real, frequency, group_input_matrices):
    positions = inputs.shape[0]
    group_list = negated_eigen_real.shape[0]
    channels = inputs.reshape(positions, group_list, -1).astype(jnp.float32)
    step_size = jnp.exp(step_logs).T
    decay_log = -negated_eigen_real[None, :, :] * step_size[:, :, None]
    magnitude = jnp.exp(decay_log + losses.T[:, :, None])
    rotation = frequency[None, :, :] * step_size[:, :, None]
    scaling = jnp.sqrt(-jnp.expm1(2.0 * decay_log))
    driven = jnp.einsum('tgc,rgpc->rtgp', channels, group_input_matrices.astype(jnp.float32), precision=lax.Precision.HIGHEST)
    return lax.associative_scan(combine_steps, (magnitude * jnp.cos(rotation), magnitude * jnp.sin(rotation), scaling * driven[0], scaling * driven[1]), axis=0)

def readout(state_real_part, state_imaginary, group_output_matrices, inputs, channel_feedthrough):
    positions = state_real_part.shape[0]
    mapped_result = jnp.einsum('fnx,njx->fnj', state_real_part, group_output_matrices[0].astype(jnp.float32), precision=lax.Precision.HIGHEST)
    mapped_result = mapped_result - jnp.einsum('fnx,njx->fnj', state_imaginary, group_output_matrices[1].astype(jnp.float32), precision=lax.Precision.HIGHEST)
    total = mapped_result.reshape(positions, -1) + channel_feedthrough * inputs.astype(jnp.float32)
    return jax.nn.gelu(total).astype(jnp.bfloat16)

def scaled_rows(values, gain):
    widened = values.astype(jnp.float32)
    factor = lax.rsqrt(lax.optimization_barrier(jnp.mean(widened * widened, axis=-1, keepdims=True)) + eps_norm)
    return (widened * factor * gain).astype(jnp.bfloat16)

def slot_table(block_routes, experts, capacity):
    flat_routes = block_routes.reshape(-1)
    onehot = (flat_routes[:, None] == jnp.arange(experts, dtype=jnp.int32)[None, :]).astype(jnp.int32)
    earlier_count = lax.optimization_barrier(jnp.sum((jnp.cumsum(onehot, axis=0) - onehot) * onehot, axis=1))
    return (flat_routes * capacity + earlier_count).astype(jnp.int32)

def fill_slots(token_rows, slot_index, slot_count, top_count):
    owner_row = jnp.zeros((slot_count,), jnp.int32).at[slot_index].set(jnp.arange(slot_index.shape[0], dtype=jnp.int32) // top_count)
    occupied = jnp.zeros((slot_count,), jnp.int32).at[slot_index].set(1)
    return jnp.where(occupied[:, None] > 0, token_rows[owner_row], jnp.zeros((), token_rows.dtype))

def expert_block(token_rows, gate_weight, up_weight, down_weight):
    gate_part = jnp.dot(token_rows, gate_weight, preferred_element_type=jnp.float32)
    up_part = jnp.dot(token_rows, up_weight, preferred_element_type=jnp.float32)
    hidden = (jax.nn.silu(gate_part) * up_part).astype(jnp.bfloat16)
    return jnp.dot(hidden, down_weight, preferred_element_type=jnp.float32)

def reference(mixer_group_input, log_step_size, extra_log_decay, negated_eigen_real, frequency, group_input_matrices, group_output_matrices, channel_feedthrough, mixer_norm_scale, mixer_output_weight, second_micro_input, expert_norm_scale, routes, chosen_expert_weight, expert_gate_weight, expert_up_weight, expert_down_weight, shared_gate_weight, shared_up_weight, shared_down_weight):
    channel_count = mixer_group_input.shape[1]
    group_list, states = negated_eigen_real.shape
    block_inputs = mixer_group_input.reshape(N_EP, TOKENS_PER_SHARD, channel_count)
    block_steps = log_step_size.reshape(group_list, N_EP, TOKENS_PER_SHARD).transpose(1, 0, 2)
    block_decay_terms = extra_log_decay.reshape(group_list, N_EP, TOKENS_PER_SHARD).transpose(1, 0, 2)

    def one_block(incoming, pieces):
        inputs, step_logs, losses = pieces
        reach_real, reach_imag, state_real_part, state_imaginary = local_states(inputs, step_logs, losses, negated_eigen_real, frequency, group_input_matrices)
        state_real_part = state_real_part + reach_real * incoming[0] - reach_imag * incoming[1]
        state_imaginary = state_imaginary + reach_real * incoming[1] + reach_imag * incoming[0]
        outputs = readout(state_real_part, state_imaginary, group_output_matrices, inputs, channel_feedthrough)
        return ((state_real_part[-1], state_imaginary[-1]), outputs)
    empty_state = jnp.zeros((group_list, states), jnp.float32)
    _, outputs = lax.scan(one_block, (empty_state, empty_state), (block_inputs, block_steps, block_decay_terms))
    ssm_out = outputs.reshape(N_EP * TOKENS_PER_SHARD, channel_count)
    normed_mix = scaled_rows(ssm_out, mixer_norm_scale)
    mixed = jnp.dot(normed_mix, mixer_output_weight, preferred_element_type=jnp.float32).astype(jnp.bfloat16)
    normed_tokens = scaled_rows(second_micro_input, expert_norm_scale)
    block_rows = normed_tokens.reshape(N_EP, TOK_EP2, D)
    slot_index = jax.vmap(lambda routes_block: slot_table(routes_block, EXPERTS, CAP))(routes.reshape(N_EP, TOK_EP2, TOP_K))
    sent = jax.vmap(lambda rows_block, slots_block: fill_slots(rows_block, slots_block, EXPERTS * CAP, TOP_K))(block_rows, slot_index)
    sent = sent.reshape(N_EP, EXPERTS, CAP, D)

    def one_expert(expert):
        arrived = lax.dynamic_index_in_dim(sent, expert, axis=1, keepdims=False).reshape(N_EP * CAP, D)
        result = expert_block(arrived, expert_gate_weight[expert], expert_up_weight[expert], expert_down_weight[expert])
        return result.astype(jnp.bfloat16).reshape(N_EP, CAP, D)
    results = lax.map(one_expert, jnp.arange(EXPERTS, dtype=jnp.int32))
    returned = results.transpose(1, 0, 2, 3).reshape(N_EP, EXPERTS * CAP, D)
    picked = jax.vmap(lambda back_block, slots_block: back_block[slots_block])(returned, slot_index)
    picked = picked.reshape(N_EP * TOK_EP2, TOP_K, D).astype(jnp.float32)
    shared = expert_block(normed_tokens, shared_gate_weight, shared_up_weight, shared_down_weight)
    moe_out = (shared + lax.optimization_barrier(jnp.sum(picked * chosen_expert_weight[:, :, None], axis=1))).astype(jnp.bfloat16)
    return (mixed, moe_out)
```

```python
import jax
import jax.numpy as jnp
from jax import lax
from jax.experimental import pallas as pl
from jax.experimental.pallas import tpu as pltpu
from jax.sharding import Mesh
from jax.sharding import PartitionSpec as P

VM = pltpu.VMEM
F32, BF16 = jnp.float32, jnp.bfloat16
NT = (((1,), (1,)), ((), ()))
EPS = 1e-06
CHUNKS = 8


def iota(shape, dim):
    return lax.broadcasted_iota(jnp.int32, shape, dim)


def vmem(count):
    return [pl.BlockSpec(memory_space=VM)] * count


def sin_cos(x):
    turns = jnp.floor(x * 0.6366197723675814 + 0.5)
    r = x - turns * 1.5703125
    r = r - turns * 4.837512969970703e-4
    r = r - turns * 7.54978995489188e-8
    q = turns.astype(jnp.int32)
    s = r * r
    sin_r = r + r * s * (-1.6666654611e-1 + s * (8.3321608736e-3 - s * 1.9515295891e-4))
    cos_r = 1.0 - 0.5 * s + s * s * (
        4.166664568298827e-2 + s * (-1.388731625493765e-3 + s * 2.443315711809948e-5)
    )
    odd = (q & 1) == 1
    a = jnp.where(odd, cos_r, sin_r)
    b = jnp.where(odd, sin_r, cos_r)
    sin_x = jnp.where((q & 2) == 2, -a, a)
    cos_x = jnp.where(((q + 1) & 2) == 2, -b, b)
    return sin_x, cos_x


def minus_expm1(y):
    small = 1.0 + y * (1.0 / 9.0)
    for n in (8, 7, 6, 5, 4, 3, 2):
        small = 1.0 + y * (1.0 / n) * small
    return jnp.where(y > -0.5, -y * small, 1.0 - jnp.exp(y))


def scan_kernel(x_ref, steps_ref, eig_ref, freq_ref, win_ref, p_re, p_im, h_re, h_im, ends_ref,
                a_re, a_im, d_re, d_im):
    positions, width = x_ref.shape
    groups = steps_ref.shape[1] // 2
    states = eig_ref.shape[1] // groups
    lanes = 128
    per = lanes // states
    channels = width // groups
    spread = (iota((channels, width), 1) % channels == iota((channels, width), 0)).astype(BF16)
    wide = jnp.dot(win_ref[...], spread, preferred_element_type=F32)
    rows = iota(wide.shape, 0) // states % groups
    wide = jnp.where(rows == iota(wide.shape, 1) // channels, wide, 0.0).astype(BF16)
    driven = lax.dot_general(x_ref[...], wide, NT, preferred_element_type=F32)
    half = groups * states
    for tile in range(half // lanes):
        at = slice(tile * lanes, (tile + 1) * lanes)
        place = iota((positions, lanes), 1) // states
        step = jnp.broadcast_to(steps_ref[:, tile * per : tile * per + 1], (positions, lanes))
        loss = jnp.broadcast_to(
            steps_ref[:, groups + tile * per : groups + tile * per + 1], (positions, lanes)
        )
        for k in range(1, per):
            g = tile * per + k
            step = jnp.where(place == k, steps_ref[:, g : g + 1], step)
            loss = jnp.where(place == k, steps_ref[:, groups + g : groups + g + 1], loss)
        decay_log = -eig_ref[:, at] * step
        magnitude = jnp.exp(decay_log + loss)
        sin_x, cos_x = sin_cos(freq_ref[:, at] * step)
        scaling = jnp.sqrt(minus_expm1(2.0 * decay_log))
        a_re[tile] = magnitude * cos_x
        a_im[tile] = magnitude * sin_x
        d_re[tile] = scaling * driven[:, at]
        d_im[tile] = scaling * driven[:, half + tile * lanes : half + (tile + 1) * lanes]
    length = positions // CHUNKS
    ends = []
    for tile in range(half // lanes):
        at = slice(tile * lanes, (tile + 1) * lanes)
        for j in range(length):
            take = pl.ds(j, CHUNKS, stride=length)
            ar, ai = a_re[tile, take, :], a_im[tile, take, :]
            dr, di = d_re[tile, take, :], d_im[tile, take, :]
            if j == 0:
                pr, pi, hr, hi = ar, ai, dr, di
            else:
                pr, pi = pr * ar - pi * ai, pr * ai + pi * ar
                hr, hi = ar * hr - ai * hi + dr, ar * hi + ai * hr + di
            p_re[j, :, at], p_im[j, :, at] = pr, pi
            h_re[j, :, at], h_im[j, :, at] = hr, hi
        er, ei, sr, si = pr[0:1], pi[0:1], hr[0:1], hi[0:1]
        for c in range(1, CHUNKS):
            ar, ai = pr[c : c + 1], pi[c : c + 1]
            er, ei = er * ar - ei * ai, er * ai + ei * ar
            sr, si = ar * sr - ai * si + hr[c : c + 1], ar * si + ai * sr + hi[c : c + 1]
        ends += [er, ei, sr, si]
    packed = jnp.concatenate(ends, axis=0)
    for b in range(ends_ref.shape[0]):
        ends_ref[b] = packed


def run_scan(x, steps, eig, freq, win, blocks):
    positions = x.shape[0]
    half = eig.shape[1]
    piece = jax.ShapeDtypeStruct((positions // CHUNKS, CHUNKS, half), F32)
    return pl.pallas_call(
        scan_kernel,
        out_shape=[piece] * 4 + [jax.ShapeDtypeStruct((blocks, half // 32, 128), F32)],
        in_specs=vmem(5),
        out_specs=vmem(5),
        scratch_shapes=[VM((half // 128, positions, 128), F32)] * 4,
        name="scan",
    )(x, steps, eig, freq, win)


def readout_kernel(where_ref, p_re, p_im, h_re, h_im, ends_ref, x_ref, wout_ref, feed_ref, out_ref,
                   turned):
    length, chunks, half = p_re.shape
    positions, width = x_ref.shape
    states = wout_ref.shape[1]
    channels = wout_ref.shape[0] // 2 // (half // states)
    index = where_ref[0]
    cr = ci = jnp.zeros((1, half), F32)
    for b in range(ends_ref.shape[0] - 1):
        end = ends_ref[b]
        ar, ai, er, ei = (
            jnp.concatenate([end[q : q + 1], end[q + 4 : q + 5]], axis=1) for q in range(4)
        )
        nr = ar * cr - ai * ci + er
        ni = ar * ci + ai * cr + ei
        keep = b < index
        cr, ci = jnp.where(keep, nr, cr), jnp.where(keep, ni, ci)
    carry_r, carry_i = [cr], [ci]
    for c in range(chunks - 1):
        ar, ai = p_re[length - 1, c : c + 1, :], p_im[length - 1, c : c + 1, :]
        cr, ci = (
            ar * cr - ai * ci + h_re[length - 1, c : c + 1, :],
            ar * ci + ai * cr + h_im[length - 1, c : c + 1, :],
        )
        carry_r.append(cr)
        carry_i.append(ci)
    cr = jnp.concatenate(carry_r, axis=0)[None]
    ci = jnp.concatenate(carry_i, axis=0)[None]
    sr = (h_re[...] + p_re[...] * cr - p_im[...] * ci).reshape(positions, half)
    si = (h_im[...] + p_re[...] * ci + p_im[...] * cr).reshape(positions, half)
    spread = (iota((states, half), 1) % states == iota((states, half), 0)).astype(BF16)
    wide = jnp.dot(wout_ref[...], spread, preferred_element_type=F32)
    rows = iota(wide.shape, 0) % width // channels
    wide = jnp.where(rows == iota(wide.shape, 1) // states, wide, 0.0)
    wr, wi = wide[:width].astype(BF16), (-wide[width:]).astype(BF16)
    nothing = jnp.zeros((128 - width, half), BF16)
    wr, wi = (jnp.concatenate([w, nothing], axis=0) for w in (wr, wi))
    total = None
    for state, w in ((sr, wr), (si, wi)):
        high = state.astype(BF16)
        low = (state - high.astype(F32)).astype(BF16)
        for part in (high, low):
            got = lax.dot_general(part, w, NT, preferred_element_type=F32)
            total = got if total is None else total + got
    for j in range(length):
        turned[pl.ds(j, chunks, stride=length), :] = total[j * chunks : (j + 1) * chunks]
    v = turned[:, :width] + feed_ref[...] * x_ref[...].astype(F32)
    v = 0.5 * v * (1.0 + jnp.tanh(0.7978845608028654 * (v + 0.044715 * (v * v * v))))
    both = positions // 2
    out_ref[...] = jnp.concatenate([v[:both], v[both:]], axis=1).astype(BF16)


def run_readout(index, pieces, ends, x, wout, feed):
    positions, width = x.shape
    return pl.pallas_call(
        readout_kernel,
        out_shape=jax.ShapeDtypeStruct((positions // 2, 2 * width), BF16),
        in_specs=[pl.BlockSpec(memory_space=pltpu.SMEM)] + vmem(8),
        out_specs=pl.BlockSpec(memory_space=VM),
        scratch_shapes=[VM((positions, 128), F32)],
        name="readout",
    )(index, *pieces, ends, x, wout, feed)


def mixed_kernel(rows_ref, scale_ref, w_ref, out_ref):
    blocks, both, lanes = rows_ref.shape
    width = lanes // 2
    total = None
    for d in range(blocks):
        v = rows_ref[d].astype(F32)
        total = v * v if total is None else total + v * v
    first = iota((both, lanes), 1) < width
    count = 1.0 / (blocks * width)
    sums = [jnp.sum(jnp.where(m, total, 0.0), axis=1, keepdims=True) for m in (first, ~first)]
    f0, f1 = (lax.rsqrt(s * count + EPS) for s in sums)
    factor = jnp.where(first, f0, f1)
    acc = [jnp.zeros((both, w_ref.shape[1]), F32)] * 2
    for d in range(blocks):
        gain = jnp.concatenate([scale_ref[d : d + 1, :]] * 2, axis=1)
        v = (rows_ref[d].astype(F32) * factor * gain).astype(BF16)
        w = w_ref[d * width : (d + 1) * width, :]
        w2 = jnp.concatenate([w, w], axis=0)
        for k, m in enumerate((first, ~first)):
            part = jnp.where(m, v, jnp.zeros_like(v))
            acc[k] = acc[k] + jnp.dot(part, w2, preferred_element_type=F32)
    out_ref[:both, :] = acc[0].astype(BF16)
    out_ref[both:, :] = acc[1].astype(BF16)


def run_mixed(rows, scale, w):
    blocks, both, lanes = rows.shape
    return pl.pallas_call(
        mixed_kernel,
        out_shape=jax.ShapeDtypeStruct((2 * both, w.shape[1]), BF16),
        in_specs=vmem(3),
        out_specs=pl.BlockSpec(memory_space=VM),
        name="mixed",
    )(rows, scale.reshape(blocks, lanes // 2), w)


def mixer_local(x, log_step, loss, eig, freq, win, blocks):
    steps = jnp.concatenate([jnp.exp(log_step), loss], axis=0).T
    return run_scan(x, steps, eig.reshape(1, -1), freq.reshape(1, -1),
                    win.reshape(-1, win.shape[-1]), blocks)


def expert_table(routes_ref, weights_ref, experts):
    top, tokens = routes_ref.shape
    expert = iota((experts, tokens), 0)
    named = jnp.zeros((experts, tokens), F32)
    gain = jnp.zeros((experts, tokens), F32)
    for k in range(top):
        hit = routes_ref[k : k + 1, :] == expert
        named = jnp.where(hit, 1.0, named)
        if weights_ref is not None:
            gain = jnp.where(hit, weights_ref[k : k + 1, :], gain)
    earlier = (iota((tokens, tokens), 0) < iota((tokens, tokens), 1)).astype(BF16)
    rank = jnp.dot(named.astype(BF16), earlier, preferred_element_type=F32)
    return jnp.where(named > 0.0, rank, -1.0), gain


def dispatch_kernel(where_ref, tokens_ref, gain_ref, routes_ref, normed_ref, sent_ref):
    tokens = tokens_ref.shape[0]
    v = tokens_ref[...].astype(F32)
    factor = lax.rsqrt(jnp.mean(v * v, axis=1, keepdims=True) + EPS)
    normed = (v * factor * gain_ref[...]).astype(BF16)
    normed_ref[...] = normed
    share = 8
    experts = sent_ref.shape[0] // share
    rank, _ = expert_table(routes_ref, None, experts)
    slot = (iota((share, tokens), 0) + where_ref[0] * share).astype(F32)
    chosen = jnp.concatenate(
        [jnp.where(rank[e : e + 1, :] == slot, 1.0, 0.0) for e in range(experts)], axis=0
    ).astype(BF16)
    sent_ref[...] = jnp.dot(chosen, normed, preferred_element_type=F32).astype(BF16)


def run_dispatch(where, tokens, gain, routes, rows):
    return pl.pallas_call(
        dispatch_kernel,
        out_shape=[
            jax.ShapeDtypeStruct(tokens.shape, BF16),
            jax.ShapeDtypeStruct((rows, tokens.shape[1]), BF16),
        ],
        in_specs=[pl.BlockSpec(memory_space=pltpu.SMEM)] + vmem(3),
        out_specs=vmem(2),
        name="dispatch",
    )(where, tokens, gain.reshape(1, -1), routes)


def choice_kernel(routes_ref, weights_ref, high_ref, low_ref):
    tokens = routes_ref.shape[1]
    share, parts = 8, 4
    experts = high_ref.shape[1] // (share * parts)
    rank, gain = expert_table(routes_ref, weights_ref, experts)
    for a in range(parts):
        slot = (iota((share, tokens), 0) + a * share).astype(F32)
        picked = jnp.concatenate(
            [
                jnp.where(rank[e : e + 1, :] == slot, gain[e : e + 1, :], 0.0)
                for e in range(experts)
            ],
            axis=0,
        ).T
        high = picked.astype(BF16)
        at = slice(a * experts * share, (a + 1) * experts * share)
        high_ref[:, at] = high
        low_ref[:, at] = (picked - high.astype(F32)).astype(BF16)


def run_choice(routes, weights, slots):
    return pl.pallas_call(
        choice_kernel,
        out_shape=[jax.ShapeDtypeStruct((routes.shape[1], slots), BF16)] * 2,
        in_specs=vmem(2),
        out_specs=vmem(2),
        name="choice",
    )(routes, weights)


def gated(rows, both):
    got = jnp.dot(rows, both, preferred_element_type=F32)
    half = both.shape[1] // 2
    gate, up = got[:, :half], got[:, half:]
    return (gate / (1.0 + jnp.exp(-gate)) * up).astype(BF16)


def hidden_kernel(rows_ref, *refs):
    *weights, out_ref = refs
    rows = rows_ref[...]
    for q, w in enumerate(weights):
        half = w.shape[1] // 2
        got = gated(rows, w[...])
        for copy in range(out_ref.shape[0]):
            out_ref[copy, :, q * half : (q + 1) * half] = got


def run_hidden(rows, weights, copies):
    half = weights[0].shape[1] // 2
    return pl.pallas_call(
        hidden_kernel,
        out_shape=jax.ShapeDtypeStruct((copies, rows.shape[0], half * len(weights)), BF16),
        in_specs=vmem(1 + len(weights)),
        out_specs=pl.BlockSpec(memory_space=VM),
        name="hidden",
    )(rows, *weights)


def down_kernel(where_ref, *refs):
    hidden, weights, out_ref, whole = refs[0], refs[1:5], refs[5], refs[6]
    sub = where_ref[0]
    lanes = weights[0].shape[1]
    for member in range(hidden.shape[0]):
        for q in range(4):
            at = pl.multiple_of((member * 4 + (sub ^ q)) * lanes, lanes)
            whole[:, pl.ds(at, lanes)] = hidden[member, :, q * lanes : (q + 1) * lanes]
    rows = whole[...]
    for q in (0, 2):
        both = jnp.concatenate([weights[q][...], weights[q + 1][...]], axis=1)
        got = jnp.dot(rows, both, preferred_element_type=F32).astype(BF16)
        out_ref[sub ^ q] = got[:, :lanes]
        out_ref[sub ^ (q + 1)] = got[:, lanes:]


def run_down(where, hidden, weights):
    rows, lanes = hidden.shape[1], weights[0].shape[1]
    return pl.pallas_call(
        down_kernel,
        out_shape=jax.ShapeDtypeStruct((4, rows, lanes), BF16),
        in_specs=[pl.BlockSpec(memory_space=pltpu.SMEM)] + vmem(5),
        out_specs=pl.BlockSpec(memory_space=VM),
        scratch_shapes=[VM((rows, weights[0].shape[0]), BF16)],
        name="down",
    )(where, hidden, *weights)


def shared_kernel(blocks_ref, w_ref, out_ref):
    blocks, tokens, lanes = blocks_ref.shape
    total = jnp.zeros((tokens, w_ref.shape[1]), F32)
    for d in range(blocks):
        total = total + jnp.dot(
            blocks_ref[d], w_ref[d * lanes : (d + 1) * lanes, :], preferred_element_type=F32
        )
    out_ref[...] = total


def run_shared(blocks, w):
    return pl.pallas_call(
        shared_kernel,
        out_shape=jax.ShapeDtypeStruct((blocks.shape[1], w.shape[1]), F32),
        in_specs=vmem(2),
        out_specs=pl.BlockSpec(memory_space=VM),
        name="shared",
    )(blocks, w)


def combine_kernel(shared_ref, back_ref, high_ref, low_ref, out_ref):
    back = back_ref[...]
    total = shared_ref[...]
    for part in (high_ref, low_ref):
        total = total + jnp.dot(part[...], back, preferred_element_type=F32)
    out_ref[...] = total.astype(BF16)


def run_combine(shared, back, high, low):
    return pl.pallas_call(
        combine_kernel,
        out_shape=jax.ShapeDtypeStruct(shared.shape, BF16),
        in_specs=vmem(4),
        out_specs=pl.BlockSpec(memory_space=VM),
        name="combine",
    )(shared, back, high, low)


TP = ("yh", "yl", "co")
SWAP = [(0, 1), (1, 0)]


def exchanged(piece):
    over = lax.ppermute(piece, "yl", SWAP)
    return (piece, lax.ppermute(piece, "co", SWAP), over, lax.ppermute(over, "co", SWAP))


def spread_out(pieces, axes):
    return lax.all_to_all(pieces, axes, split_axis=0, concat_axis=0, tiled=True)


def on_device(
    mixer_group_input,
    log_step_size,
    extra_log_decay,
    negated_eigen_real,
    frequency,
    group_input_matrices,
    group_output_matrices,
    channel_feedthrough,
    mixer_norm_scale,
    mixer_output_weight,
    second_micro_input,
    expert_norm_scale,
    routes,
    chosen_expert_weight,
    expert_gate_weight,
    expert_up_weight,
    expert_down_weight,
    shared_gate_weight,
    shared_up_weight,
    shared_down_weight,
):
    blocks = lax.axis_size("ep")
    tokens, width = second_micro_input.shape
    sub = 2 * lax.axis_index("yl") + lax.axis_index("co")
    where = jnp.stack([sub, lax.axis_index("ep")]).astype(jnp.int32)
    routes = routes.T
    gates = exchanged(jnp.concatenate([expert_gate_weight[0], expert_up_weight[0]], axis=1))
    normed, sent = run_dispatch(where, second_micro_input, expert_norm_scale, routes, blocks * 8)
    arrived = spread_out(sent.reshape(blocks, 8, width), "ep").reshape(blocks * 8, width)
    downs = exchanged(expert_down_weight[0])

    *pieces, ends = mixer_local(
        mixer_group_input,
        log_step_size,
        extra_log_decay,
        negated_eigen_real,
        frequency,
        group_input_matrices,
        blocks,
    )
    ends = spread_out(ends, "ep")
    ssm_out = run_readout(
        where[1:],
        pieces,
        ends,
        mixer_group_input,
        group_output_matrices.reshape(-1, group_output_matrices.shape[-1]),
        channel_feedthrough.reshape(1, -1),
    )
    whole_rows = lax.all_gather(ssm_out, TP, axis=0)
    mixed = run_mixed(whole_rows, mixer_norm_scale, mixer_output_weight)

    shared_gates = jnp.concatenate([shared_gate_weight, shared_up_weight], axis=1)
    shared_hidden = run_hidden(normed, [shared_gates], 1)[0]
    shared = run_shared(lax.all_gather(shared_hidden, TP, axis=0), shared_down_weight)
    high, low = run_choice(routes, chosen_expert_weight.T, blocks * 32)

    hidden = run_hidden(arrived, gates, lax.axis_size("yh"))
    hidden = spread_out(hidden, "yh")
    results = run_down(where, hidden, downs)
    results = results.reshape(4 * blocks, 8, -1)
    back = spread_out(results, ("yl", "co", "ep")).reshape(blocks * 32, -1)
    return (mixed, run_combine(shared, back, high, low))


def solution(mesh):
    finer = Mesh(
        mesh.devices.reshape(mesh.shape["ep"], mesh.shape["tp"] // 4, 2, 2), ("ep", *TP)
    )
    return jax.shard_map(
        on_device,
        mesh=finer,
        in_specs=(
            P("ep", TP),
            P(TP, "ep"),
            P(TP, "ep"),
            P(TP, None),
            P(TP, None),
            P(None, TP, None, None),
            P(None, TP, None, None),
            P(TP),
            P(),
            P(None, TP),
            P("ep", None),
            P(),
            P("ep", None),
            P("ep", None),
            P("ep", None, TP),
            P("ep", None, TP),
            P("ep", None, TP),
            P(None, TP),
            P(None, TP),
            P(None, TP),
        ),
        out_specs=(P("ep", TP), P("ep", TP)),
        check_vma=False,
    )
```

```python
import jax
import jax.numpy as jnp
from jax import lax
from jax.experimental import pallas as pl
from jax.experimental.pallas import tpu as pltpu
from jax.sharding import Mesh
from jax.sharding import PartitionSpec as P


VM = pltpu.VMEM
F32, BF16 = jnp.float32, jnp.bfloat16
NT = (((1,), (1,)), ((), ()))
EPS = 1e-06
CHUNKS = 8


def iota(shape, dim):
    return lax.broadcasted_iota(jnp.int32, shape, dim)


def vmem(count):
    return [pl.BlockSpec(memory_space=VM)] * count


def sin_cos(x):
    turns = jnp.floor(x * 0.6366197723675814 + 0.5)
    r = x - turns * 1.5703125
    r = r - turns * 4.837512969970703e-4
    r = r - turns * 7.54978995489188e-8
    q = turns.astype(jnp.int32)
    s = r * r
    sin_r = r + r * s * (-1.6666654611e-1 + s * (8.3321608736e-3 - s * 1.9515295891e-4))
    cos_r = 1.0 - 0.5 * s + s * s * (
        4.166664568298827e-2 + s * (-1.388731625493765e-3 + s * 2.443315711809948e-5)
    )
    odd = (q & 1) == 1
    a = jnp.where(odd, cos_r, sin_r)
    b = jnp.where(odd, sin_r, cos_r)
    sin_x = jnp.where((q & 2) == 2, -a, a)
    cos_x = jnp.where(((q + 1) & 2) == 2, -b, b)
    return sin_x, cos_x


def minus_expm1(y):
    small = 1.0 + y * (1.0 / 9.0)
    for n in (8, 7, 6, 5, 4, 3, 2):
        small = 1.0 + y * (1.0 / n) * small
    return jnp.where(y > -0.5, -y * small, 1.0 - jnp.exp(y))


def flat(ref):
    return jnp.concatenate([ref[g : g + 1, :] for g in range(ref.shape[0])], axis=1)


def block_diagonal(ref, groups):
    rows, states = ref.shape
    width = rows // 2
    half = groups * states
    repeat = (iota((states, half), 1) % states == iota((states, half), 0)).astype(BF16)
    wide = jnp.dot(ref[...], repeat, preferred_element_type=F32)
    group = iota(wide.shape, 0) % width // (width // groups)
    wide = jnp.where(group == iota(wide.shape, 1) // states, wide, 0.0)
    return wide[:width], wide[width:]


def scan_part(x_ref, log_ref, loss_ref, eig_ref, freq_ref, win_ref, feed_ref,
              p_re, p_im, h_re, h_im, through_ref, a_re, a_im, d_re, d_im):
    _, positions = x_ref.shape
    groups, states = eig_ref.shape
    lanes = 128
    per = lanes // states
    x = x_ref[...].astype(F32).T
    through_ref[...] = x * feed_ref[...]
    steps = jnp.concatenate([jnp.exp(log_ref[...]), loss_ref[...]], axis=0).T
    eig, freq = flat(eig_ref), flat(freq_ref)
    x = x.astype(BF16)
    driven = [
        jnp.dot(x, w.astype(BF16), preferred_element_type=F32)
        for w in block_diagonal(win_ref, groups)
    ]
    half = groups * states
    for tile in range(half // lanes):
        at = slice(tile * lanes, (tile + 1) * lanes)
        place = iota((positions, lanes), 1) // states
        step = jnp.broadcast_to(steps[:, tile * per : tile * per + 1], (positions, lanes))
        loss = jnp.broadcast_to(
            steps[:, groups + tile * per : groups + tile * per + 1], (positions, lanes)
        )
        for k in range(1, per):
            g = tile * per + k
            step = jnp.where(place == k, steps[:, g : g + 1], step)
            loss = jnp.where(place == k, steps[:, groups + g : groups + g + 1], loss)
        decay_log = -eig[:, at] * step
        magnitude = jnp.exp(decay_log + loss)
        sin_x, cos_x = sin_cos(freq[:, at] * step)
        scaling = jnp.sqrt(minus_expm1(2.0 * decay_log))
        a_re[tile] = magnitude * cos_x
        a_im[tile] = magnitude * sin_x
        d_re[tile] = scaling * driven[0][:, at]
        d_im[tile] = scaling * driven[1][:, at]
    length = positions // CHUNKS
    ends = []
    for tile in range(half // lanes):
        at = slice(tile * lanes, (tile + 1) * lanes)
        for j in range(length):
            take = pl.ds(j, CHUNKS, stride=length)
            ar, ai = a_re[tile, take, :], a_im[tile, take, :]
            dr, di = d_re[tile, take, :], d_im[tile, take, :]
            if j == 0:
                pr, pi, hr, hi = ar, ai, dr, di
            else:
                pr, pi = pr * ar - pi * ai, pr * ai + pi * ar
                hr, hi = ar * hr - ai * hi + dr, ar * hi + ai * hr + di
            p_re[j, :, at], p_im[j, :, at] = pr, pi
            h_re[j, :, at], h_im[j, :, at] = hr, hi
        er, ei, sr, si = pr[0:1], pi[0:1], hr[0:1], hi[0:1]
        for c in range(1, CHUNKS):
            ar, ai = pr[c : c + 1], pi[c : c + 1]
            er, ei = er * ar - ei * ai, er * ai + ei * ar
            sr, si = ar * sr - ai * si + hr[c : c + 1], ar * si + ai * sr + hi[c : c + 1]
        ends += [er, ei, sr, si]
    ends = jnp.concatenate(ends, axis=0)
    high = ends.astype(BF16)
    return jnp.concatenate([high, (ends - high.astype(F32)).astype(BF16)], axis=1)


def readout_kernel(p_re, p_im, h_re, h_im, ends_ref, through_ref, wout_ref, out_ref, turned):
    length, chunks, half = p_re.shape
    positions, width = through_ref.shape
    index = lax.axis_index("ep")
    cr = ci = jnp.zeros((1, half), F32)
    for b in range(ends_ref.shape[0] - 1):
        end = ends_ref[b].astype(F32)
        end = end[:, :128] + end[:, 128:]
        ar, ai, er, ei = (
            jnp.concatenate([end[q : q + 1], end[q + 4 : q + 5]], axis=1) for q in range(4)
        )
        nr = ar * cr - ai * ci + er
        ni = ar * ci + ai * cr + ei
        keep = b < index
        cr, ci = jnp.where(keep, nr, cr), jnp.where(keep, ni, ci)
    carry_r, carry_i = [cr], [ci]
    for c in range(chunks - 1):
        ar, ai = p_re[length - 1, c : c + 1, :], p_im[length - 1, c : c + 1, :]
        cr, ci = (
            ar * cr - ai * ci + h_re[length - 1, c : c + 1, :],
            ar * ci + ai * cr + h_im[length - 1, c : c + 1, :],
        )
        carry_r.append(cr)
        carry_i.append(ci)
    cr = jnp.concatenate(carry_r, axis=0)[None]
    ci = jnp.concatenate(carry_i, axis=0)[None]
    sr = (h_re[...] + p_re[...] * cr - p_im[...] * ci).reshape(positions, half)
    si = (h_im[...] + p_re[...] * ci + p_im[...] * cr).reshape(positions, half)
    wr, wi = block_diagonal(wout_ref, half // wout_ref.shape[1])
    wr, wi = wr.astype(BF16), (-wi).astype(BF16)
    nothing = jnp.zeros((128 - width, half), BF16)
    wr, wi = (jnp.concatenate([w, nothing], axis=0) for w in (wr, wi))
    total = None
    for state, w in ((sr, wr), (si, wi)):
        high = state.astype(BF16)
        low = (state - high.astype(F32)).astype(BF16)
        for part in (high, low):
            got = lax.dot_general(part, w, NT, preferred_element_type=F32)
            total = got if total is None else total + got
    for j in range(length):
        turned[pl.ds(j, chunks, stride=length), :] = total[j * chunks : (j + 1) * chunks]
    v = turned[:, :width] + through_ref[...]
    v = 0.5 * v * (1.0 + jnp.tanh(0.7978845608028654 * (v + 0.044715 * (v * v * v))))
    both = positions // 2
    out_ref[...] = jnp.concatenate([v[:both], v[both:]], axis=1).astype(BF16)


def run_readout(pieces, ends, through, wout):
    positions, width = through.shape
    return pl.pallas_call(
        readout_kernel,
        out_shape=jax.ShapeDtypeStruct((positions // 2, 2 * width), BF16),
        in_specs=vmem(7),
        out_specs=pl.BlockSpec(memory_space=VM),
        scratch_shapes=[VM((positions, 128), F32)],
        name="readout",
    )(*pieces, ends, through, wout)


def mixed_kernel(rows_ref, scale_ref, w_ref, out_ref):
    blocks, both, lanes = rows_ref.shape
    width = lanes // 2
    total = None
    for d in range(blocks):
        v = rows_ref[d].astype(F32)
        total = v * v if total is None else total + v * v
    first = iota((both, lanes), 1) < width
    count = 1.0 / (blocks * width)
    sums = [jnp.sum(jnp.where(m, total, 0.0), axis=1, keepdims=True) for m in (first, ~first)]
    f0, f1 = (lax.rsqrt(s * count + EPS) for s in sums)
    factor = jnp.where(first, f0, f1)
    acc = [jnp.zeros((both, w_ref.shape[1]), F32)] * 2
    for d in range(blocks):
        gain = jnp.concatenate([scale_ref[d : d + 1, :]] * 2, axis=1)
        v = (rows_ref[d].astype(F32) * factor * gain).astype(BF16)
        w = w_ref[d * width : (d + 1) * width, :]
        w2 = jnp.concatenate([w, w], axis=0)
        for k, m in enumerate((first, ~first)):
            part = jnp.where(m, v, jnp.zeros_like(v))
            acc[k] = acc[k] + jnp.dot(part, w2, preferred_element_type=F32)
    out_ref[:both, :] = acc[0].astype(BF16)
    out_ref[both:, :] = acc[1].astype(BF16)


def run_mixed(rows, scale, w):
    blocks, both, lanes = rows.shape
    return pl.pallas_call(
        mixed_kernel,
        out_shape=jax.ShapeDtypeStruct((2 * both, w.shape[1]), BF16),
        in_specs=vmem(3),
        out_specs=pl.BlockSpec(memory_space=VM),
        name="mixed",
    )(rows, scale.reshape(blocks, lanes // 2), w)


def expert_table(routes_ref, weights_ref, experts):
    top, tokens = routes_ref.shape
    expert = iota((experts, tokens), 0)
    named = jnp.zeros((experts, tokens), F32)
    gain = jnp.zeros((experts, tokens), F32)
    for k in range(top):
        hit = routes_ref[k : k + 1, :] == expert
        named = jnp.where(hit, 1.0, named)
        if weights_ref is not None:
            gain = jnp.where(hit, weights_ref[k : k + 1, :], gain)
    earlier = (iota((tokens, tokens), 0) < iota((tokens, tokens), 1)).astype(BF16)
    rank = jnp.dot(named.astype(BF16), earlier, preferred_element_type=F32)
    return jnp.where(named > 0.0, rank, -1.0), gain


def own_sub():
    return 2 * lax.axis_index("yl") + lax.axis_index("co")


def first_kernel(tokens_ref, gain_ref, routes_ref, *refs):
    scan_in, (normed_ref, sent_ref), scan_out = refs[:7], refs[7:9], refs[9:]
    ends = scan_part(*scan_in, *scan_out)
    tokens, width = tokens_ref.shape
    v = tokens_ref[...].astype(F32)
    factor = lax.rsqrt(jnp.mean(v * v, axis=1, keepdims=True) + EPS)
    normed = (v * factor * gain_ref[...]).astype(BF16)
    normed_ref[...] = normed
    share = ends.shape[0]
    experts = sent_ref.shape[0] // share
    rank, _ = expert_table(routes_ref, None, experts)
    slot = (iota((share, tokens), 0) + own_sub() * share).astype(F32)
    chosen = jnp.concatenate(
        [jnp.where(rank[e : e + 1, :] == slot, 1.0, 0.0) for e in range(experts)], axis=0
    ).astype(BF16)
    sent_ref[:, :width] = jnp.dot(chosen, normed, preferred_element_type=F32).astype(BF16)
    for e in range(experts):
        sent_ref[e * share : (e + 1) * share, width:] = ends


def run_first(tokens, gain, routes, blocks, x, log_step, loss, eig, freq, win, feed):
    width, positions = x.shape
    half = eig.size
    piece = jax.ShapeDtypeStruct((positions // CHUNKS, CHUNKS, half), F32)
    return pl.pallas_call(
        first_kernel,
        out_shape=[
            jax.ShapeDtypeStruct(tokens.shape, BF16),
            jax.ShapeDtypeStruct((blocks * half // 32, tokens.shape[1] + 256), BF16),
        ]
        + [piece] * 4
        + [jax.ShapeDtypeStruct((positions, width), F32)],
        in_specs=vmem(10),
        out_specs=vmem(7),
        scratch_shapes=[VM((half // 128, positions, 128), F32)] * 4,
        name="first",
    )(tokens, gain.reshape(1, -1), routes, x, log_step, loss, eig, freq, win, feed)


def choice_kernel(routes_ref, weights_ref, high_ref, low_ref):
    tokens = routes_ref.shape[1]
    share, parts = 8, 4
    experts = high_ref.shape[1] // (share * parts)
    rank, gain = expert_table(routes_ref, weights_ref, experts)
    for a in range(parts):
        slot = (iota((share, tokens), 0) + a * share).astype(F32)
        picked = jnp.concatenate(
            [
                jnp.where(rank[e : e + 1, :] == slot, gain[e : e + 1, :], 0.0)
                for e in range(experts)
            ],
            axis=0,
        ).T
        high = picked.astype(BF16)
        at = slice(a * experts * share, (a + 1) * experts * share)
        high_ref[:, at] = high
        low_ref[:, at] = (picked - high.astype(F32)).astype(BF16)


def run_choice(routes, weights, slots):
    return pl.pallas_call(
        choice_kernel,
        out_shape=[jax.ShapeDtypeStruct((routes.shape[1], slots), BF16)] * 2,
        in_specs=vmem(2),
        out_specs=vmem(2),
        name="choice",
    )(routes, weights)


def gated(got):
    half = got.shape[1] // 2
    gate, up = got[:, :half], got[:, half:]
    return (gate / (1.0 + jnp.exp(-gate)) * up).astype(BF16)


def hidden_kernel(rows_ref, *refs):
    *weights, out_ref = refs
    rows = rows_ref[:, : weights[0].shape[0]]
    for q, w in enumerate(weights):
        half = w.shape[1] // 2
        got = gated(jnp.dot(rows, w[...], preferred_element_type=F32))
        for copy in range(out_ref.shape[0]):
            out_ref[copy, :, q * half : (q + 1) * half] = got


def shared_hidden_kernel(rows_ref, gate_ref, up_ref, out_ref):
    both = jnp.concatenate([gate_ref[...], up_ref[...]], axis=1)
    got = gated(jnp.dot(rows_ref[...], both, preferred_element_type=F32))
    out_ref[...] = got


def run_shared_hidden(rows, gate, up):
    return pl.pallas_call(
        shared_hidden_kernel,
        out_shape=jax.ShapeDtypeStruct((rows.shape[0], gate.shape[1]), BF16),
        in_specs=vmem(3),
        out_specs=pl.BlockSpec(memory_space=VM),
        name="shared_hidden",
    )(rows, gate, up)


def run_hidden(rows, weights, copies):
    half = weights[0].shape[1] // 2
    return pl.pallas_call(
        hidden_kernel,
        out_shape=jax.ShapeDtypeStruct((copies, rows.shape[0], half * len(weights)), BF16),
        in_specs=vmem(1 + len(weights)),
        out_specs=pl.BlockSpec(memory_space=VM),
        name="hidden",
    )(rows, *weights)


def down_kernel(*refs):
    hidden, weights, out_ref, whole = refs[0], refs[1:5], refs[5], refs[6]
    sub = own_sub()
    lanes = weights[0].shape[1]
    for member in range(hidden.shape[0]):
        for q in range(4):
            at = pl.multiple_of((member * 4 + (sub ^ q)) * lanes, lanes)
            whole[:, pl.ds(at, lanes)] = hidden[member, :, q * lanes : (q + 1) * lanes]
    rows = whole[...]
    for q in (0, 2):
        both = jnp.concatenate([weights[q][...], weights[q + 1][...]], axis=1)
        got = jnp.dot(rows, both, preferred_element_type=F32).astype(BF16)
        out_ref[sub ^ q] = got[:, :lanes]
        out_ref[sub ^ (q + 1)] = got[:, lanes:]


def run_down(hidden, weights):
    rows, lanes = hidden.shape[1], weights[0].shape[1]
    return pl.pallas_call(
        down_kernel,
        out_shape=jax.ShapeDtypeStruct((4, rows, lanes), BF16),
        in_specs=vmem(5),
        out_specs=pl.BlockSpec(memory_space=VM),
        scratch_shapes=[VM((rows, weights[0].shape[0]), BF16)],
        name="down",
    )(hidden, *weights)


def shared_kernel(blocks_ref, w_ref, out_ref):
    blocks, tokens, lanes = blocks_ref.shape
    total = jnp.zeros((tokens, w_ref.shape[1]), F32)
    for d in range(blocks):
        total = total + jnp.dot(
            blocks_ref[d], w_ref[d * lanes : (d + 1) * lanes, :], preferred_element_type=F32
        )
    out_ref[...] = total


def run_shared(blocks, w):
    return pl.pallas_call(
        shared_kernel,
        out_shape=jax.ShapeDtypeStruct((blocks.shape[1], w.shape[1]), F32),
        in_specs=vmem(2),
        out_specs=pl.BlockSpec(memory_space=VM),
        name="shared",
    )(blocks, w)


def combine_kernel(shared_ref, back_ref, high_ref, low_ref, out_ref):
    back = back_ref[...]
    total = shared_ref[...]
    for part in (high_ref, low_ref):
        total = total + jnp.dot(part[...], back, preferred_element_type=F32)
    out_ref[...] = total.astype(BF16)


def run_combine(shared, back, high, low):
    return pl.pallas_call(
        combine_kernel,
        out_shape=jax.ShapeDtypeStruct(shared.shape, BF16),
        in_specs=vmem(4),
        out_specs=pl.BlockSpec(memory_space=VM),
        name="combine",
    )(shared, back, high, low)


TP = ("yh", "yl", "co")
SWAP = [(0, 1), (1, 0)]


def exchanged(piece):
    over = lax.ppermute(piece, "yl", SWAP)
    core = lax.ppermute(piece, "co", SWAP)
    both = lax.ppermute(over, "co", SWAP)
    return (piece, core, over, both)


def spread_out(pieces, axes):
    return lax.all_to_all(pieces, axes, split_axis=0, concat_axis=0, tiled=True)


def on_device(
    mixer_group_input,
    log_step_size,
    extra_log_decay,
    negated_eigen_real,
    frequency,
    group_input_matrices,
    group_output_matrices,
    channel_feedthrough,
    mixer_norm_scale,
    mixer_output_weight,
    second_micro_input,
    expert_norm_scale,
    routes,
    chosen_expert_weight,
    expert_gate_weight,
    expert_up_weight,
    expert_down_weight,
    shared_gate_weight,
    shared_up_weight,
    shared_down_weight,
):
    blocks = lax.axis_size("ep")
    width = second_micro_input.shape[1]
    routes = routes.T
    normed, sent, *pieces, through = run_first(
        second_micro_input,
        expert_norm_scale,
        routes,
        blocks,
        mixer_group_input.T,
        log_step_size,
        extra_log_decay,
        negated_eigen_real,
        frequency,
        group_input_matrices.swapaxes(2, 3).reshape(-1, frequency.shape[1]),
        channel_feedthrough.reshape(1, -1),
    )
    arrived = spread_out(sent.reshape(blocks, 8, -1), "ep")
    both = jnp.concatenate([expert_gate_weight[0], expert_up_weight[0]], axis=1)
    gates = exchanged(both)
    downs = exchanged(expert_down_weight[0])

    shared_hidden = run_shared_hidden(normed, shared_gate_weight, shared_up_weight)
    shared_rows = lax.all_gather(shared_hidden, TP, axis=0)
    shared = run_shared(shared_rows, shared_down_weight)

    ssm_out = run_readout(
        pieces,
        arrived[:, :, width:],
        through,
        group_output_matrices.reshape(-1, frequency.shape[1]),
    )
    whole_rows = lax.all_gather(ssm_out, TP, axis=0)
    mixed = run_mixed(whole_rows, mixer_norm_scale, mixer_output_weight)
    high, low = run_choice(routes, chosen_expert_weight.T, blocks * 32)

    hidden = run_hidden(arrived.reshape(blocks * 8, -1), gates, lax.axis_size("yh"))
    hidden = spread_out(hidden, "yh")
    results = run_down(hidden, downs).reshape(4 * blocks, 8, -1)
    back = spread_out(results, ("yl", "co", "ep")).reshape(blocks * 32, -1)
    return (mixed, run_combine(shared, back, high, low))


def solution(mesh):
    finer = Mesh(
        mesh.devices.reshape(mesh.shape["ep"], mesh.shape["tp"] // 4, 2, 2), ("ep", *TP)
    )
    return jax.shard_map(
        on_device,
        mesh=finer,
        in_specs=(
            P("ep", TP),
            P(TP, "ep"),
            P(TP, "ep"),
            P(TP, None),
            P(TP, None),
            P(None, TP, None, None),
            P(None, TP, None, None),
            P(TP),
            P(),
            P(None, TP),
            P("ep", None),
            P(),
            P("ep", None),
            P("ep", None),
            P("ep", None, TP),
            P("ep", None, TP),
            P("ep", None, TP),
            P(None, TP),
            P(None, TP),
            P(None, TP),
        ),
        out_specs=(P("ep", TP), P("ep", TP)),
        check_vma=False,
    )
```

```python
import jax
import jax.numpy as jnp
from jax import lax
from jax.experimental import pallas as pl
from jax.experimental.pallas import tpu as pltpu
from jax.sharding import Mesh
from jax.sharding import PartitionSpec as P


VM = pltpu.VMEM
F32, BF16 = jnp.float32, jnp.bfloat16
NT = (((1,), (1,)), ((), ()))
EPS = 1e-06
CHUNKS = 8


def iota(shape, dim):
    return lax.broadcasted_iota(jnp.int32, shape, dim)


def vmem(count):
    return [pl.BlockSpec(memory_space=VM)] * count


def sin_cos(x):
    turns = jnp.floor(x * 0.6366197723675814 + 0.5)
    r = x - turns * 1.5703125
    r = r - turns * 4.837512969970703e-4
    r = r - turns * 7.54978995489188e-8
    q = turns.astype(jnp.int32)
    s = r * r
    sin_r = r + r * s * (-1.6666654611e-1 + s * (8.3321608736e-3 - s * 1.9515295891e-4))
    cos_r = 1.0 - 0.5 * s + s * s * (
        4.166664568298827e-2 + s * (-1.388731625493765e-3 + s * 2.443315711809948e-5)
    )
    odd = (q & 1) == 1
    a = jnp.where(odd, cos_r, sin_r)
    b = jnp.where(odd, sin_r, cos_r)
    sin_x = jnp.where((q & 2) == 2, -a, a)
    cos_x = jnp.where(((q + 1) & 2) == 2, -b, b)
    return sin_x, cos_x


def minus_expm1(y):
    small = 1.0 + y * (1.0 / 9.0)
    for n in (8, 7, 6, 5, 4, 3, 2):
        small = 1.0 + y * (1.0 / n) * small
    return jnp.where(y > -0.5, -y * small, 1.0 - jnp.exp(y))


def flat(ref):
    return jnp.concatenate([ref[g : g + 1, :] for g in range(ref.shape[0])], axis=1)


def block_diagonal(ref, groups):
    rows, states = ref.shape
    width = rows // 2
    half = groups * states
    repeat = (iota((states, half), 1) % states == iota((states, half), 0)).astype(BF16)
    wide = jnp.dot(ref[...], repeat, preferred_element_type=F32)
    group = iota(wide.shape, 0) % width // (width // groups)
    wide = jnp.where(group == iota(wide.shape, 1) // states, wide, 0.0)
    return wide[:width], wide[width:]


def scan_part(x_ref, log_ref, loss_ref, eig_ref, freq_ref, win_ref, feed_ref,
              p_re, p_im, h_re, h_im, through_ref, a_re, a_im, d_re, d_im):
    _, positions = x_ref.shape
    groups, states = eig_ref.shape
    lanes = 128
    per = lanes // states
    x = x_ref[...].astype(F32).T
    through_ref[...] = x * feed_ref[...]
    steps = jnp.concatenate([jnp.exp(log_ref[...]), loss_ref[...]], axis=0).T
    eig, freq = flat(eig_ref), flat(freq_ref)
    x = x.astype(BF16)
    driven = [
        jnp.dot(x, w.astype(BF16), preferred_element_type=F32)
        for w in block_diagonal(win_ref, groups)
    ]
    half = groups * states
    for tile in range(half // lanes):
        at = slice(tile * lanes, (tile + 1) * lanes)
        place = iota((positions, lanes), 1) // states
        step = jnp.broadcast_to(steps[:, tile * per : tile * per + 1], (positions, lanes))
        loss = jnp.broadcast_to(
            steps[:, groups + tile * per : groups + tile * per + 1], (positions, lanes)
        )
        for k in range(1, per):
            g = tile * per + k
            step = jnp.where(place == k, steps[:, g : g + 1], step)
            loss = jnp.where(place == k, steps[:, groups + g : groups + g + 1], loss)
        decay_log = -eig[:, at] * step
        magnitude = jnp.exp(decay_log + loss)
        sin_x, cos_x = sin_cos(freq[:, at] * step)
        scaling = jnp.sqrt(minus_expm1(2.0 * decay_log))
        a_re[tile] = magnitude * cos_x
        a_im[tile] = magnitude * sin_x
        d_re[tile] = scaling * driven[0][:, at]
        d_im[tile] = scaling * driven[1][:, at]
    length = positions // CHUNKS
    ends = []
    for tile in range(half // lanes):
        at = slice(tile * lanes, (tile + 1) * lanes)
        for j in range(length):
            take = pl.ds(j, CHUNKS, stride=length)
            ar, ai = a_re[tile, take, :], a_im[tile, take, :]
            dr, di = d_re[tile, take, :], d_im[tile, take, :]
            if j == 0:
                pr, pi, hr, hi = ar, ai, dr, di
            else:
                pr, pi = pr * ar - pi * ai, pr * ai + pi * ar
                hr, hi = ar * hr - ai * hi + dr, ar * hi + ai * hr + di
            p_re[j, :, at], p_im[j, :, at] = pr, pi
            h_re[j, :, at], h_im[j, :, at] = hr, hi
        er, ei, sr, si = pr[0:1], pi[0:1], hr[0:1], hi[0:1]
        for c in range(1, CHUNKS):
            ar, ai = pr[c : c + 1], pi[c : c + 1]
            er, ei = er * ar - ei * ai, er * ai + ei * ar
            sr, si = ar * sr - ai * si + hr[c : c + 1], ar * si + ai * sr + hi[c : c + 1]
        ends += [er, ei, sr, si]
    ends = jnp.concatenate(ends, axis=0)
    high = ends.astype(BF16)
    return jnp.concatenate([high, (ends - high.astype(F32)).astype(BF16)], axis=1)


def readout_part(p_re, p_im, h_re, h_im, ends_ref, through_ref, wout_ref, turned):
    length, chunks, half = p_re.shape
    positions, width = through_ref.shape
    index = lax.axis_index("ep")
    cr = ci = jnp.zeros((1, half), F32)
    for b in range(ends_ref.shape[0] - 1):
        end = ends_ref[b, :, ends_ref.shape[2] - 256 :].astype(F32)
        end = end[:, :128] + end[:, 128:]
        ar, ai, er, ei = (
            jnp.concatenate([end[q : q + 1], end[q + 4 : q + 5]], axis=1) for q in range(4)
        )
        nr = ar * cr - ai * ci + er
        ni = ar * ci + ai * cr + ei
        keep = b < index
        cr, ci = jnp.where(keep, nr, cr), jnp.where(keep, ni, ci)
    carry_r, carry_i = [cr], [ci]
    for c in range(chunks - 1):
        ar, ai = p_re[length - 1, c : c + 1, :], p_im[length - 1, c : c + 1, :]
        cr, ci = (
            ar * cr - ai * ci + h_re[length - 1, c : c + 1, :],
            ar * ci + ai * cr + h_im[length - 1, c : c + 1, :],
        )
        carry_r.append(cr)
        carry_i.append(ci)
    cr = jnp.concatenate(carry_r, axis=0)[None]
    ci = jnp.concatenate(carry_i, axis=0)[None]
    sr = (h_re[...] + p_re[...] * cr - p_im[...] * ci).reshape(positions, half)
    si = (h_im[...] + p_re[...] * ci + p_im[...] * cr).reshape(positions, half)
    wr, wi = block_diagonal(wout_ref, half // wout_ref.shape[1])
    wr, wi = wr.astype(BF16), (-wi).astype(BF16)
    nothing = jnp.zeros((128 - width, half), BF16)
    wr, wi = (jnp.concatenate([w, nothing], axis=0) for w in (wr, wi))
    total = None
    for state, w in ((sr, wr), (si, wi)):
        high = state.astype(BF16)
        low = (state - high.astype(F32)).astype(BF16)
        for part in (high, low):
            got = lax.dot_general(part, w, NT, preferred_element_type=F32)
            total = got if total is None else total + got
    for j in range(length):
        turned[pl.ds(j, chunks, stride=length), :] = total[j * chunks : (j + 1) * chunks]
    v = turned[:, :width] + through_ref[...]
    v = 0.5 * v * (1.0 + jnp.tanh(0.7978845608028654 * (v + 0.044715 * (v * v * v))))
    both = positions // 2
    return jnp.concatenate([v[:both], v[both:]], axis=1).astype(BF16)


def block_of(ref, member, part):
    rows = ref.shape[1] // 2
    lanes = 128
    return jnp.concatenate(
        [
            ref[member, part * rows : (part + 1) * rows, i * lanes : (i + 1) * lanes]
            for i in range(ref.shape[2] // lanes)
        ],
        axis=0,
    )


def third_kernel(*refs):
    pieces, (scale_ref, w_ref, down_ref, mixed_ref, shared_ref) = refs[:4], refs[4:]
    sub = own_sub()
    members = pieces[0].shape[0]
    places = [(m, q) for m in range(members) for q in range(4)]
    blocks = [block_of(pieces[q], m, 0) for m, q in places]
    both, lanes = blocks[0].shape
    width = lanes // 2
    total = None
    for v in blocks:
        v = v.astype(F32)
        total = v * v if total is None else total + v * v
    first = iota((both, lanes), 1) < width
    count = 1.0 / (len(places) * width)
    sums = [jnp.sum(jnp.where(m, total, 0.0), axis=1, keepdims=True) for m in (first, ~first)]
    f0, f1 = (lax.rsqrt(s * count + EPS) for s in sums)
    factor = jnp.where(first, f0, f1)
    acc = [jnp.zeros((both, w_ref.shape[1]), F32)] * 2
    shared = jnp.zeros(shared_ref.shape, F32)
    for (m, q), block in zip(places, blocks):
        d = m * 4 + (sub ^ q)
        gain = jnp.concatenate([scale_ref[pl.ds(d, 1), :]] * 2, axis=1)
        v = (block.astype(F32) * factor * gain).astype(BF16)
        w = w_ref[pl.ds(pl.multiple_of(d * width, width), width), :]
        w2 = jnp.concatenate([w, w], axis=0)
        for k, half in enumerate((first, ~first)):
            part = jnp.where(half, v, jnp.zeros_like(v))
            acc[k] = acc[k] + jnp.dot(part, w2, preferred_element_type=F32)
        shared = shared + jnp.dot(
            block_of(pieces[q], m, 1),
            down_ref[pl.ds(pl.multiple_of(d * lanes, lanes), lanes), :],
            preferred_element_type=F32,
        )
    mixed_ref[:both, :] = acc[0].astype(BF16)
    mixed_ref[both:, :] = acc[1].astype(BF16)
    shared_ref[...] = shared


def run_third(pieces, scale, w, down, positions, tokens):
    lanes = w.shape[1]
    return pl.pallas_call(
        third_kernel,
        out_shape=[
            jax.ShapeDtypeStruct((positions, lanes), BF16),
            jax.ShapeDtypeStruct((tokens, lanes), F32),
        ],
        in_specs=vmem(7),
        out_specs=vmem(2),
        name="third",
    )(*pieces, scale.reshape(pieces[0].shape[0] * 4, -1), w, down)


def expert_table(routes_ref, weights_ref, experts):
    top, tokens = routes_ref.shape
    expert = iota((experts, tokens), 0)
    named = jnp.zeros((experts, tokens), F32)
    gain = jnp.zeros((experts, tokens), F32)
    for k in range(top):
        hit = routes_ref[k : k + 1, :] == expert
        named = jnp.where(hit, 1.0, named)
        if weights_ref is not None:
            gain = jnp.where(hit, weights_ref[k : k + 1, :], gain)
    earlier = (iota((tokens, tokens), 0) < iota((tokens, tokens), 1)).astype(BF16)
    rank = jnp.dot(named.astype(BF16), earlier, preferred_element_type=F32)
    return jnp.where(named > 0.0, rank, -1.0), gain


def own_sub():
    return 2 * lax.axis_index("yl") + lax.axis_index("co")


def first_kernel(tokens_ref, gain_ref, routes_ref, *refs):
    scan_in, (normed_ref, sent_ref), scan_out = refs[:7], refs[7:9], refs[9:]
    ends = scan_part(*scan_in, *scan_out)
    tokens, width = tokens_ref.shape
    v = tokens_ref[...].astype(F32)
    factor = lax.rsqrt(jnp.mean(v * v, axis=1, keepdims=True) + EPS)
    normed = (v * factor * gain_ref[...]).astype(BF16)
    normed_ref[...] = normed
    share = ends.shape[0]
    experts = sent_ref.shape[0] // share
    rank, _ = expert_table(routes_ref, None, experts)
    slot = (iota((share, tokens), 0) + own_sub() * share).astype(F32)
    chosen = jnp.concatenate(
        [jnp.where(rank[e : e + 1, :] == slot, 1.0, 0.0) for e in range(experts)], axis=0
    ).astype(BF16)
    sent_ref[:, :width] = jnp.dot(chosen, normed, preferred_element_type=F32).astype(BF16)
    for e in range(experts):
        sent_ref[e * share : (e + 1) * share, width:] = ends


def run_first(tokens, gain, routes, blocks, x, log_step, loss, eig, freq, win, feed):
    width, positions = x.shape
    half = eig.size
    piece = jax.ShapeDtypeStruct((positions // CHUNKS, CHUNKS, half), F32)
    return pl.pallas_call(
        first_kernel,
        out_shape=[
            jax.ShapeDtypeStruct(tokens.shape, BF16),
            jax.ShapeDtypeStruct((blocks * half // 32, tokens.shape[1] + 256), BF16),
        ]
        + [piece] * 4
        + [jax.ShapeDtypeStruct((positions, width), F32)],
        in_specs=vmem(10),
        out_specs=vmem(7),
        scratch_shapes=[VM((half // 128, positions, 128), F32)] * 4,
        name="first",
    )(tokens, gain.reshape(1, -1), routes, x, log_step, loss, eig, freq, win, feed)


def choice_kernel(routes_ref, weights_ref, high_ref, low_ref):
    tokens = routes_ref.shape[1]
    share, parts = 8, 4
    experts = high_ref.shape[1] // (share * parts)
    rank, gain = expert_table(routes_ref, weights_ref, experts)
    for a in range(parts):
        slot = (iota((share, tokens), 0) + a * share).astype(F32)
        picked = jnp.concatenate(
            [
                jnp.where(rank[e : e + 1, :] == slot, gain[e : e + 1, :], 0.0)
                for e in range(experts)
            ],
            axis=0,
        ).T
        high = picked.astype(BF16)
        at = slice(a * experts * share, (a + 1) * experts * share)
        high_ref[:, at] = high
        low_ref[:, at] = (picked - high.astype(F32)).astype(BF16)


def run_choice(routes, weights, slots):
    return pl.pallas_call(
        choice_kernel,
        out_shape=[jax.ShapeDtypeStruct((routes.shape[1], slots), BF16)] * 2,
        in_specs=vmem(2),
        out_specs=vmem(2),
        name="choice",
    )(routes, weights)


def gated(got):
    half = got.shape[1] // 2
    gate, up = got[:, :half], got[:, half:]
    return (gate / (1.0 + jnp.exp(-gate)) * up).astype(BF16)


def second_kernel(arrived_ref, extra_ref, *refs):
    gates, ups, readout_in, (out_ref, turned) = refs[:4], refs[4:8], refs[8:14], refs[14:]
    mix = readout_part(*readout_in[:4], arrived_ref, *readout_in[4:], turned)
    blocks, share, _ = arrived_ref.shape
    rows = arrived_ref[:, :, : gates[0].shape[0]].reshape(blocks * share, -1)
    copies, _, wide = out_ref.shape
    lanes = mix.shape[1]
    for q, (gate, up) in enumerate(zip(gates, ups)):
        both = jnp.concatenate([gate[...], up[...]], axis=1)
        got = gated(jnp.dot(rows, both, preferred_element_type=F32))
        for copy in range(copies):
            out_ref[copy, : blocks * share, q * lanes : (q + 1) * lanes] = got
    at = blocks * share
    for item in (mix, extra_ref[...]):
        part = item.shape[0] * lanes // wide
        for i in range(wide // lanes):
            for copy in range(copies):
                out_ref[copy, at : at + part, i * lanes : (i + 1) * lanes] = item[
                    i * part : (i + 1) * part
                ]
        at += part


def run_second(arrived, extra, gates, ups, pieces, through, wout, copies):
    blocks, share, _ = arrived.shape
    wide = 4 * gates[0].shape[1]
    rows = blocks * share + (through.size + extra.size) // wide
    return pl.pallas_call(
        second_kernel,
        out_shape=jax.ShapeDtypeStruct((copies, rows, wide), BF16),
        in_specs=vmem(16),
        out_specs=pl.BlockSpec(memory_space=VM),
        scratch_shapes=[VM((through.shape[0], 128), F32)],
        name="second",
    )(arrived, extra, *gates, *ups, *pieces, through, wout)


def shared_hidden_kernel(rows_ref, gate_ref, up_ref, out_ref):
    both = jnp.concatenate([gate_ref[...], up_ref[...]], axis=1)
    got = gated(jnp.dot(rows_ref[...], both, preferred_element_type=F32))
    out_ref[...] = got


def run_shared_hidden(rows, gate, up):
    return pl.pallas_call(
        shared_hidden_kernel,
        out_shape=jax.ShapeDtypeStruct((rows.shape[0], gate.shape[1]), BF16),
        in_specs=vmem(3),
        out_specs=pl.BlockSpec(memory_space=VM),
        name="shared_hidden",
    )(rows, gate, up)


def down_kernel(*refs):
    hidden, weights, out_ref, whole = refs[0], refs[1:5], refs[5], refs[6]
    sub = own_sub()
    lanes = weights[0].shape[1]
    for member in range(hidden.shape[0]):
        for q in range(4):
            at = pl.multiple_of((member * 4 + (sub ^ q)) * lanes, lanes)
            whole[:, pl.ds(at, lanes)] = hidden[member, : whole.shape[0], q * lanes : (q + 1) * lanes]
    rows = whole[...]
    for q in (0, 2):
        both = jnp.concatenate([weights[q][...], weights[q + 1][...]], axis=1)
        got = jnp.dot(rows, both, preferred_element_type=F32).astype(BF16)
        out_ref[sub ^ q] = got[:, :lanes]
        out_ref[sub ^ (q + 1)] = got[:, lanes:]


def run_down(hidden, weights, rows):
    lanes = weights[0].shape[1]
    return pl.pallas_call(
        down_kernel,
        out_shape=jax.ShapeDtypeStruct((4, rows, lanes), BF16),
        in_specs=vmem(5),
        out_specs=pl.BlockSpec(memory_space=VM),
        scratch_shapes=[VM((rows, weights[0].shape[0]), BF16)],
        name="down",
    )(hidden, *weights)


def combine_kernel(shared_ref, back_ref, high_ref, low_ref, out_ref):
    back = back_ref[...]
    total = shared_ref[...]
    for part in (high_ref, low_ref):
        total = total + jnp.dot(part[...], back, preferred_element_type=F32)
    out_ref[...] = total.astype(BF16)


def run_combine(shared, back, high, low):
    return pl.pallas_call(
        combine_kernel,
        out_shape=jax.ShapeDtypeStruct(shared.shape, BF16),
        in_specs=vmem(4),
        out_specs=pl.BlockSpec(memory_space=VM),
        name="combine",
    )(shared, back, high, low)


TP = ("yh", "yl", "co")
SWAP = [(0, 1), (1, 0)]


def exchanged(piece):
    over = lax.ppermute(piece, "yl", SWAP)
    core = lax.ppermute(piece, "co", SWAP)
    both = lax.ppermute(over, "co", SWAP)
    return (piece, core, over, both)


def spread_out(pieces, axes):
    return lax.all_to_all(pieces, axes, split_axis=0, concat_axis=0, tiled=True)


def on_device(
    mixer_group_input,
    log_step_size,
    extra_log_decay,
    negated_eigen_real,
    frequency,
    group_input_matrices,
    group_output_matrices,
    channel_feedthrough,
    mixer_norm_scale,
    mixer_output_weight,
    second_micro_input,
    expert_norm_scale,
    routes,
    chosen_expert_weight,
    expert_gate_weight,
    expert_up_weight,
    expert_down_weight,
    shared_gate_weight,
    shared_up_weight,
    shared_down_weight,
):
    blocks = lax.axis_size("ep")
    routes = routes.T
    normed, sent, *pieces, through = run_first(
        second_micro_input,
        expert_norm_scale,
        routes,
        blocks,
        mixer_group_input.T,
        log_step_size,
        extra_log_decay,
        negated_eigen_real,
        frequency,
        group_input_matrices.swapaxes(2, 3).reshape(-1, frequency.shape[1]),
        channel_feedthrough.reshape(1, -1),
    )
    arrived = spread_out(sent.reshape(blocks, 8, -1), "ep")
    gates = exchanged(expert_gate_weight[0])
    ups = exchanged(expert_up_weight[0])
    downs = exchanged(expert_down_weight[0])
    shared_hidden = run_shared_hidden(normed, shared_gate_weight, shared_up_weight)
    high, low = run_choice(routes, chosen_expert_weight.T, blocks * 32)

    hidden = run_second(
        arrived,
        shared_hidden,
        gates,
        ups,
        pieces,
        through,
        group_output_matrices.reshape(-1, frequency.shape[1]),
        lax.axis_size("yh"),
    )
    hidden = spread_out(hidden, "yh")
    results = run_down(hidden, downs, blocks * 8).reshape(4 * blocks, 8, -1)
    back = spread_out(results, ("yl", "co", "ep")).reshape(blocks * 32, -1)

    own = hidden[:, blocks * 8 :]
    core = lax.ppermute(own, "co", SWAP)
    over = lax.ppermute(own, "yl", SWAP)
    both = lax.ppermute(core, "yl", SWAP)
    mixed, shared = run_third(
        (own, core, over, both),
        mixer_norm_scale,
        mixer_output_weight,
        shared_down_weight,
        through.shape[0],
        routes.shape[1],
    )
    return (mixed, run_combine(shared, back, high, low))


def solution(mesh):
    finer = Mesh(
        mesh.devices.reshape(mesh.shape["ep"], mesh.shape["tp"] // 4, 2, 2), ("ep", *TP)
    )
    return jax.shard_map(
        on_device,
        mesh=finer,
        in_specs=(
            P("ep", TP),
            P(TP, "ep"),
            P(TP, "ep"),
            P(TP, None),
            P(TP, None),
            P(None, TP, None, None),
            P(None, TP, None, None),
            P(TP),
            P(),
            P(None, TP),
            P("ep", None),
            P(),
            P("ep", None),
            P("ep", None),
            P("ep", None, TP),
            P("ep", None, TP),
            P("ep", None, TP),
            P(None, TP),
            P(None, TP),
            P(None, TP),
        ),
        out_specs=(P("ep", TP), P("ep", TP)),
        check_vma=False,
    )
```

```python
import jax
import jax.numpy as jnp
from jax import lax
from jax.experimental import pallas as pl
from jax.experimental.pallas import tpu as pltpu
from jax.sharding import Mesh
from jax.sharding import PartitionSpec as P


VM = pltpu.VMEM
F32, BF16 = jnp.float32, jnp.bfloat16
NT = (((1,), (1,)), ((), ()))
EPS = 1e-06
CHUNKS = 8


def iota(shape, dim):
    return lax.broadcasted_iota(jnp.int32, shape, dim)


def vmem(count):
    return [pl.BlockSpec(memory_space=VM)] * count


def held(*arrays):
    return [pltpu.with_memory_space_constraint(a, VM) for a in arrays]


def sin_cos(x):
    turns = jnp.floor(x * 0.6366197723675814 + 0.5)
    r = x - turns * 1.5703125
    r = r - turns * 4.837512969970703e-4
    r = r - turns * 7.54978995489188e-8
    q = turns.astype(jnp.int32)
    s = r * r
    sin_r = r + r * s * (-1.6666654611e-1 + s * (8.3321608736e-3 - s * 1.9515295891e-4))
    cos_r = 1.0 - 0.5 * s + s * s * (
        4.166664568298827e-2 + s * (-1.388731625493765e-3 + s * 2.443315711809948e-5)
    )
    odd = (q & 1) == 1
    a = jnp.where(odd, cos_r, sin_r)
    b = jnp.where(odd, sin_r, cos_r)
    sin_x = jnp.where((q & 2) == 2, -a, a)
    cos_x = jnp.where(((q + 1) & 2) == 2, -b, b)
    return sin_x, cos_x


def minus_expm1(y):
    small = 1.0 + y * (1.0 / 9.0)
    for n in (8, 7, 6, 5, 4, 3, 2):
        small = 1.0 + y * (1.0 / n) * small
    return jnp.where(y > -0.5, -y * small, 1.0 - jnp.exp(y))


def flat(ref):
    return jnp.concatenate([ref[g : g + 1, :] for g in range(ref.shape[0])], axis=1)


def block_diagonal(ref, groups):
    rows, states = ref.shape
    width = rows // 2
    half = groups * states
    repeat = (iota((states, half), 1) % states == iota((states, half), 0)).astype(BF16)
    wide = jnp.dot(ref[...], repeat, preferred_element_type=F32)
    group = iota(wide.shape, 0) % width // (width // groups)
    wide = jnp.where(group == iota(wide.shape, 1) // states, wide, 0.0)
    return wide[:width], wide[width:]


def scan_part(x_ref, log_ref, loss_ref, eig_ref, freq_ref, win_ref, feed_ref,
              p_re, p_im, h_re, h_im, through_ref, a_re, a_im, d_re, d_im):
    _, positions = x_ref.shape
    groups, states = eig_ref.shape
    lanes = 128
    per = lanes // states
    x = x_ref[...].astype(F32).T
    through_ref[...] = x * feed_ref[...]
    steps = jnp.concatenate([jnp.exp(log_ref[...]), loss_ref[...]], axis=0).T
    eig, freq = flat(eig_ref), flat(freq_ref)
    x = x.astype(BF16)
    driven = [
        jnp.dot(x, w.astype(BF16), preferred_element_type=F32)
        for w in block_diagonal(win_ref, groups)
    ]
    half = groups * states
    for tile in range(half // lanes):
        at = slice(tile * lanes, (tile + 1) * lanes)
        place = iota((positions, lanes), 1) // states
        step = jnp.broadcast_to(steps[:, tile * per : tile * per + 1], (positions, lanes))
        loss = jnp.broadcast_to(
            steps[:, groups + tile * per : groups + tile * per + 1], (positions, lanes)
        )
        for k in range(1, per):
            g = tile * per + k
            step = jnp.where(place == k, steps[:, g : g + 1], step)
            loss = jnp.where(place == k, steps[:, groups + g : groups + g + 1], loss)
        decay_log = -eig[:, at] * step
        magnitude = jnp.exp(decay_log + loss)
        sin_x, cos_x = sin_cos(freq[:, at] * step)
        scaling = jnp.sqrt(minus_expm1(2.0 * decay_log))
        a_re[tile] = magnitude * cos_x
        a_im[tile] = magnitude * sin_x
        d_re[tile] = scaling * driven[0][:, at]
        d_im[tile] = scaling * driven[1][:, at]
    length = positions // CHUNKS
    ends = []
    for tile in range(half // lanes):
        at = slice(tile * lanes, (tile + 1) * lanes)
        for j in range(length):
            take = pl.ds(j, CHUNKS, stride=length)
            ar, ai = a_re[tile, take, :], a_im[tile, take, :]
            dr, di = d_re[tile, take, :], d_im[tile, take, :]
            if j == 0:
                pr, pi, hr, hi = ar, ai, dr, di
            else:
                pr, pi = pr * ar - pi * ai, pr * ai + pi * ar
                hr, hi = ar * hr - ai * hi + dr, ar * hi + ai * hr + di
            p_re[j, :, at], p_im[j, :, at] = pr, pi
            h_re[j, :, at], h_im[j, :, at] = hr, hi
        er, ei, sr, si = pr[0:1], pi[0:1], hr[0:1], hi[0:1]
        for c in range(1, CHUNKS):
            ar, ai = pr[c : c + 1], pi[c : c + 1]
            er, ei = er * ar - ei * ai, er * ai + ei * ar
            sr, si = ar * sr - ai * si + hr[c : c + 1], ar * si + ai * sr + hi[c : c + 1]
        ends += [er, ei, sr, si]
    ends = jnp.concatenate(ends, axis=0)
    high = ends.astype(BF16)
    return jnp.concatenate([high, (ends - high.astype(F32)).astype(BF16)], axis=1)


def readout_part(p_re, p_im, h_re, h_im, ends_ref, through_ref, wout_ref, turned):
    length, chunks, half = p_re.shape
    positions, width = through_ref.shape
    index = lax.axis_index("ep")
    cr = ci = jnp.zeros((1, half), F32)
    for b in range(ends_ref.shape[0] - 1):
        end = ends_ref[b, :, ends_ref.shape[2] - 256 :].astype(F32)
        end = end[:, :128] + end[:, 128:]
        ar, ai, er, ei = (
            jnp.concatenate([end[q : q + 1], end[q + 4 : q + 5]], axis=1) for q in range(4)
        )
        nr = ar * cr - ai * ci + er
        ni = ar * ci + ai * cr + ei
        keep = b < index
        cr, ci = jnp.where(keep, nr, cr), jnp.where(keep, ni, ci)
    carry_r, carry_i = [cr], [ci]
    for c in range(chunks - 1):
        ar, ai = p_re[length - 1, c : c + 1, :], p_im[length - 1, c : c + 1, :]
        cr, ci = (
            ar * cr - ai * ci + h_re[length - 1, c : c + 1, :],
            ar * ci + ai * cr + h_im[length - 1, c : c + 1, :],
        )
        carry_r.append(cr)
        carry_i.append(ci)
    cr = jnp.concatenate(carry_r, axis=0)[None]
    ci = jnp.concatenate(carry_i, axis=0)[None]
    sr = (h_re[...] + p_re[...] * cr - p_im[...] * ci).reshape(positions, half)
    si = (h_im[...] + p_re[...] * ci + p_im[...] * cr).reshape(positions, half)
    wr, wi = block_diagonal(wout_ref, half // wout_ref.shape[1])
    wr, wi = wr.astype(BF16), (-wi).astype(BF16)
    nothing = jnp.zeros((128 - width, half), BF16)
    wr, wi = (jnp.concatenate([w, nothing], axis=0) for w in (wr, wi))
    total = None
    for state, w in ((sr, wr), (si, wi)):
        high = state.astype(BF16)
        low = (state - high.astype(F32)).astype(BF16)
        for part in (high, low):
            got = lax.dot_general(part, w, NT, preferred_element_type=F32)
            total = got if total is None else total + got
    for j in range(length):
        turned[pl.ds(j, chunks, stride=length), :] = total[j * chunks : (j + 1) * chunks]
    v = turned[:, :width] + through_ref[...]
    v = 0.5 * v * (1.0 + jnp.tanh(0.7978845608028654 * (v + 0.044715 * (v * v * v))))
    both = positions // 2
    return jnp.concatenate([v[:both], v[both:]], axis=1).astype(BF16)


def block_of(ref, member, part):
    rows = ref.shape[1] // 2
    lanes = 128
    return jnp.concatenate(
        [
            ref[member, part * rows : (part + 1) * rows, i * lanes : (i + 1) * lanes]
            for i in range(ref.shape[2] // lanes)
        ],
        axis=0,
    )


def third_kernel(*refs):
    pieces, (scale_ref, w_ref, down_ref, mixed_ref, shared_ref, gains) = refs[:4], refs[4:]
    for d in range(gains.shape[0]):
        part = scale_ref[:, d * gains.shape[1] : (d + 1) * gains.shape[1]]
        gains[d : d + 1, :] = part
    sub = own_sub()
    members = pieces[0].shape[0]
    places = [(m, q) for m in range(members) for q in range(4)]
    blocks = [block_of(pieces[q], m, 0) for m, q in places]
    both, lanes = blocks[0].shape
    width = lanes // 2
    total = None
    for v in blocks:
        v = v.astype(F32)
        total = v * v if total is None else total + v * v
    first = iota((both, lanes), 1) < width
    count = 1.0 / (len(places) * width)
    sums = [jnp.sum(jnp.where(m, total, 0.0), axis=1, keepdims=True) for m in (first, ~first)]
    f0, f1 = (lax.rsqrt(s * count + EPS) for s in sums)
    factor = jnp.where(first, f0, f1)
    acc = [jnp.zeros((both, w_ref.shape[1]), F32)] * 2
    shared = jnp.zeros(shared_ref.shape, F32)
    for (m, q), block in zip(places, blocks):
        d = m * 4 + (sub ^ q)
        gain = jnp.concatenate([gains[pl.ds(d, 1), :]] * 2, axis=1)
        v = (block.astype(F32) * factor * gain).astype(BF16)
        w = w_ref[pl.ds(pl.multiple_of(d * width, width), width), :]
        w2 = jnp.concatenate([w, w], axis=0)
        for k, half in enumerate((first, ~first)):
            part = jnp.where(half, v, jnp.zeros_like(v))
            acc[k] = acc[k] + jnp.dot(part, w2, preferred_element_type=F32)
        shared = shared + jnp.dot(
            block_of(pieces[q], m, 1),
            down_ref[pl.ds(pl.multiple_of(d * lanes, lanes), lanes), :],
            preferred_element_type=F32,
        )
    mixed_ref[:both, :] = acc[0].astype(BF16)
    mixed_ref[both:, :] = acc[1].astype(BF16)
    shared_ref[...] = shared


def run_third(pieces, scale, w, down, positions, tokens):
    lanes = w.shape[1]
    return pl.pallas_call(
        third_kernel,
        out_shape=[
            jax.ShapeDtypeStruct((positions, lanes), BF16),
            jax.ShapeDtypeStruct((tokens, lanes), F32),
        ],
        in_specs=vmem(7),
        out_specs=vmem(2),
        scratch_shapes=[VM((pieces[0].shape[0] * 4, scale.size // pieces[0].shape[0] // 4), F32)],
        name="third",
    )(pieces[0], *held(*pieces[1:]), scale.reshape(1, -1), w, down)


def expert_table(routes_ref, weights_ref, experts):
    top, tokens = routes_ref.shape
    expert = iota((experts, tokens), 0)
    named = jnp.zeros((experts, tokens), F32)
    gain = jnp.zeros((experts, tokens), F32)
    for k in range(top):
        hit = routes_ref[k : k + 1, :] == expert
        named = jnp.where(hit, 1.0, named)
        if weights_ref is not None:
            gain = jnp.where(hit, weights_ref[k : k + 1, :], gain)
    earlier = (iota((tokens, tokens), 0) < iota((tokens, tokens), 1)).astype(BF16)
    rank = jnp.dot(named.astype(BF16), earlier, preferred_element_type=F32)
    return jnp.where(named > 0.0, rank, -1.0), gain


def own_sub():
    return 2 * lax.axis_index("yl") + lax.axis_index("co")


def first_kernel(tokens_ref, gain_ref, routes_ref, *refs):
    scan_in, (normed_ref, sent_ref), scan_out = refs[:7], refs[7:9], refs[9:]
    ends = scan_part(*scan_in, *scan_out)
    tokens, width = tokens_ref.shape
    v = tokens_ref[...].astype(F32)
    factor = lax.rsqrt(jnp.mean(v * v, axis=1, keepdims=True) + EPS)
    normed = (v * factor * gain_ref[...]).astype(BF16)
    normed_ref[...] = normed
    share = ends.shape[0]
    experts = sent_ref.shape[0] // share
    rank, _ = expert_table(routes_ref, None, experts)
    slot = (iota((share, tokens), 0) + own_sub() * share).astype(F32)
    chosen = jnp.concatenate(
        [jnp.where(rank[e : e + 1, :] == slot, 1.0, 0.0) for e in range(experts)], axis=0
    ).astype(BF16)
    sent_ref[:, :width] = jnp.dot(chosen, normed, preferred_element_type=F32).astype(BF16)
    for e in range(experts):
        sent_ref[e * share : (e + 1) * share, width:] = ends


def run_first(tokens, gain, routes, blocks, x, log_step, loss, eig, freq, win, feed):
    width, positions = x.shape
    half = eig.size
    piece = jax.ShapeDtypeStruct((positions // CHUNKS, CHUNKS, half), F32)
    return pl.pallas_call(
        first_kernel,
        out_shape=[
            jax.ShapeDtypeStruct(tokens.shape, BF16),
            jax.ShapeDtypeStruct((blocks * half // 32, tokens.shape[1] + 256), BF16),
        ]
        + [piece] * 4
        + [jax.ShapeDtypeStruct((positions, width), F32)],
        in_specs=vmem(10),
        out_specs=vmem(7),
        scratch_shapes=[VM((half // 128, positions, 128), F32)] * 4,
        name="first",
    )(tokens, gain.reshape(1, -1), routes, x, log_step, loss, eig, freq, win, feed)


def choice_kernel(routes_ref, weights_ref, high_ref, low_ref):
    tokens = routes_ref.shape[1]
    share, parts = 8, 4
    experts = high_ref.shape[1] // (share * parts)
    rank, gain = expert_table(routes_ref, weights_ref, experts)
    for a in range(parts):
        slot = (iota((share, tokens), 0) + a * share).astype(F32)
        picked = jnp.concatenate(
            [
                jnp.where(rank[e : e + 1, :] == slot, gain[e : e + 1, :], 0.0)
                for e in range(experts)
            ],
            axis=0,
        ).T
        high = picked.astype(BF16)
        at = slice(a * experts * share, (a + 1) * experts * share)
        high_ref[:, at] = high
        low_ref[:, at] = (picked - high.astype(F32)).astype(BF16)


def run_choice(routes, weights, slots):
    return pl.pallas_call(
        choice_kernel,
        out_shape=[jax.ShapeDtypeStruct((routes.shape[1], slots), BF16)] * 2,
        in_specs=vmem(2),
        out_specs=vmem(2),
        name="choice",
    )(routes, weights)


def gated(got):
    half = got.shape[1] // 2
    gate, up = got[:, :half], got[:, half:]
    return (gate / (1.0 + jnp.exp(-gate)) * up).astype(BF16)


def second_kernel(arrived_ref, extra_ref, *refs):
    gates, ups, readout_in, (out_ref, turned) = refs[:4], refs[4:8], refs[8:14], refs[14:]
    mix = readout_part(*readout_in[:4], arrived_ref, *readout_in[4:], turned)
    blocks, share, _ = arrived_ref.shape
    rows = arrived_ref[:, :, : gates[0].shape[0]].reshape(blocks * share, -1)
    copies, _, wide = out_ref.shape
    lanes = mix.shape[1]
    for q, (gate, up) in enumerate(zip(gates, ups)):
        both = jnp.concatenate([gate[...], up[...]], axis=1)
        got = gated(jnp.dot(rows, both, preferred_element_type=F32))
        for copy in range(copies):
            out_ref[copy, : blocks * share, q * lanes : (q + 1) * lanes] = got
    at = blocks * share
    for item in (mix, extra_ref[...]):
        part = item.shape[0] * lanes // wide
        for i in range(wide // lanes):
            for copy in range(copies):
                out_ref[copy, at : at + part, i * lanes : (i + 1) * lanes] = item[
                    i * part : (i + 1) * part
                ]
        at += part


def run_second(arrived, extra, gates, ups, pieces, through, wout, copies):
    blocks, share, _ = arrived.shape
    wide = 4 * gates[0].shape[1]
    rows = blocks * share + (through.size + extra.size) // wide
    return pl.pallas_call(
        second_kernel,
        out_shape=jax.ShapeDtypeStruct((copies, rows, wide), BF16),
        in_specs=vmem(16),
        out_specs=pl.BlockSpec(memory_space=VM),
        scratch_shapes=[VM((through.shape[0], 128), F32)],
        name="second",
    )(*held(arrived), extra, *gates, *ups, *pieces, through, wout)


def shared_hidden_kernel(rows_ref, gate_ref, up_ref, out_ref):
    both = jnp.concatenate([gate_ref[...], up_ref[...]], axis=1)
    got = gated(jnp.dot(rows_ref[...], both, preferred_element_type=F32))
    out_ref[...] = got


def run_shared_hidden(rows, gate, up):
    return pl.pallas_call(
        shared_hidden_kernel,
        out_shape=jax.ShapeDtypeStruct((rows.shape[0], gate.shape[1]), BF16),
        in_specs=vmem(3),
        out_specs=pl.BlockSpec(memory_space=VM),
        name="shared_hidden",
    )(rows, gate, up)


def down_kernel(*refs):
    hidden, weights, (out_ref, rest_ref, whole) = refs[0], refs[1:5], refs[5:]
    rest_ref[...] = hidden[:, whole.shape[0] :, :]
    sub = own_sub()
    lanes = weights[0].shape[1]
    for member in range(hidden.shape[0]):
        for q in range(4):
            at = pl.multiple_of((member * 4 + (sub ^ q)) * lanes, lanes)
            whole[:, pl.ds(at, lanes)] = hidden[member, : whole.shape[0], q * lanes : (q + 1) * lanes]
    rows = whole[...]
    for q in (0, 2):
        both = jnp.concatenate([weights[q][...], weights[q + 1][...]], axis=1)
        got = jnp.dot(rows, both, preferred_element_type=F32).astype(BF16)
        out_ref[sub ^ q] = got[:, :lanes]
        out_ref[sub ^ (q + 1)] = got[:, lanes:]


def run_down(hidden, weights, rows):
    lanes = weights[0].shape[1]
    return pl.pallas_call(
        down_kernel,
        out_shape=[
            jax.ShapeDtypeStruct((4, rows, lanes), BF16),
            jax.ShapeDtypeStruct(
                (hidden.shape[0], hidden.shape[1] - rows, hidden.shape[2]), BF16
            ),
        ],
        in_specs=vmem(5),
        out_specs=vmem(2),
        scratch_shapes=[VM((rows, weights[0].shape[0]), BF16)],
        name="down",
    )(*held(hidden), *weights)


def combine_kernel(shared_ref, back_ref, high_ref, low_ref, out_ref):
    back = back_ref[...]
    total = shared_ref[...]
    for part in (high_ref, low_ref):
        total = total + jnp.dot(part[...], back, preferred_element_type=F32)
    out_ref[...] = total.astype(BF16)


def run_combine(shared, back, high, low):
    return pl.pallas_call(
        combine_kernel,
        out_shape=jax.ShapeDtypeStruct(shared.shape, BF16),
        in_specs=vmem(4),
        out_specs=pl.BlockSpec(memory_space=VM),
        name="combine",
    )(shared, *held(back), high, low)


TP = ("yh", "yl", "co")
SWAP = [(0, 1), (1, 0)]


def exchanged(piece):
    over = lax.ppermute(piece, "yl", SWAP)
    core = lax.ppermute(piece, "co", SWAP)
    both = lax.ppermute(over, "co", SWAP)
    return (piece, core, over, both)


def spread_out(pieces, axes):
    return lax.all_to_all(pieces, axes, split_axis=0, concat_axis=0, tiled=True)


def on_device(
    mixer_group_input,
    log_step_size,
    extra_log_decay,
    negated_eigen_real,
    frequency,
    group_input_matrices,
    group_output_matrices,
    channel_feedthrough,
    mixer_norm_scale,
    mixer_output_weight,
    second_micro_input,
    expert_norm_scale,
    routes,
    chosen_expert_weight,
    expert_gate_weight,
    expert_up_weight,
    expert_down_weight,
    shared_gate_weight,
    shared_up_weight,
    shared_down_weight,
):
    blocks = lax.axis_size("ep")
    routes = routes.T
    normed, sent, *pieces, through = run_first(
        second_micro_input,
        expert_norm_scale,
        routes,
        blocks,
        mixer_group_input.T,
        log_step_size,
        extra_log_decay,
        negated_eigen_real,
        frequency,
        group_input_matrices.swapaxes(2, 3).reshape(-1, frequency.shape[1]),
        channel_feedthrough.reshape(1, -1),
    )
    arrived = spread_out(sent.reshape(blocks, 8, -1), "ep")
    gates = exchanged(expert_gate_weight[0])
    ups = exchanged(expert_up_weight[0])
    downs = exchanged(expert_down_weight[0])
    shared_hidden = run_shared_hidden(normed, shared_gate_weight, shared_up_weight)
    high, low = run_choice(routes, chosen_expert_weight.T, blocks * 32)

    hidden = run_second(
        arrived,
        shared_hidden,
        gates,
        ups,
        pieces,
        through,
        group_output_matrices.reshape(-1, frequency.shape[1]),
        lax.axis_size("yh"),
    )
    hidden = spread_out(hidden, "yh")
    results, own = run_down(hidden, downs, blocks * 8)
    results = results.reshape(4 * blocks, 8, -1)
    back = spread_out(results, ("yl", "co", "ep")).reshape(blocks * 32, -1)

    core = lax.ppermute(own, "co", SWAP)
    over = lax.ppermute(own, "yl", SWAP)
    both = lax.ppermute(over, "co", SWAP)
    mixed, shared = run_third(
        (own, core, over, both),
        mixer_norm_scale,
        mixer_output_weight,
        shared_down_weight,
        through.shape[0],
        routes.shape[1],
    )
    return (mixed, run_combine(shared, back, high, low))


def solution(mesh):
    finer = Mesh(
        mesh.devices.reshape(mesh.shape["ep"], mesh.shape["tp"] // 4, 2, 2), ("ep", *TP)
    )
    return jax.shard_map(
        on_device,
        mesh=finer,
        in_specs=(
            P("ep", TP),
            P(TP, "ep"),
            P(TP, "ep"),
            P(TP, None),
            P(TP, None),
            P(None, TP, None, None),
            P(None, TP, None, None),
            P(TP),
            P(),
            P(None, TP),
            P("ep", None),
            P(),
            P("ep", None),
            P("ep", None),
            P("ep", None, TP),
            P("ep", None, TP),
            P("ep", None, TP),
            P(None, TP),
            P(None, TP),
            P(None, TP),
        ),
        out_specs=(P("ep", TP), P("ep", TP)),
        check_vma=False,
    )
```

```python
import jax
import jax.numpy as jnp
from jax import lax
from jax.experimental import pallas as pl
from jax.experimental.pallas import tpu as pltpu
from jax.sharding import Mesh
from jax.sharding import PartitionSpec as P


VM = pltpu.VMEM
F32, BF16 = jnp.float32, jnp.bfloat16
NT = (((1,), (1,)), ((), ()))
EPS = 1e-06
CHUNKS = 8


def iota(shape, dim):
    return lax.broadcasted_iota(jnp.int32, shape, dim)


def vmem(count):
    return [pl.BlockSpec(memory_space=VM)] * count


def held(*arrays):
    return [pltpu.with_memory_space_constraint(a, VM) for a in arrays]


def sin_cos(x):
    turns = jnp.floor(x * 0.6366197723675814 + 0.5)
    r = x - turns * 1.5703125
    r = r - turns * 4.837512969970703e-4
    r = r - turns * 7.54978995489188e-8
    q = turns.astype(jnp.int32)
    s = r * r
    sin_r = r + r * s * (-1.6666654611e-1 + s * (8.3321608736e-3 - s * 1.9515295891e-4))
    cos_r = 1.0 - 0.5 * s + s * s * (
        4.166664568298827e-2 + s * (-1.388731625493765e-3 + s * 2.443315711809948e-5)
    )
    odd = (q & 1) == 1
    a = jnp.where(odd, cos_r, sin_r)
    b = jnp.where(odd, sin_r, cos_r)
    sin_x = jnp.where((q & 2) == 2, -a, a)
    cos_x = jnp.where(((q + 1) & 2) == 2, -b, b)
    return sin_x, cos_x


def minus_expm1(y):
    small = 1.0 + y * (1.0 / 9.0)
    for n in (8, 7, 6, 5, 4, 3, 2):
        small = 1.0 + y * (1.0 / n) * small
    return jnp.where(y > -0.5, -y * small, 1.0 - jnp.exp(y))


def flat(ref):
    return jnp.concatenate([ref[g : g + 1, :] for g in range(ref.shape[0])], axis=1)


def block_diagonal(ref, groups):
    rows, states = ref.shape
    width = rows // 2
    half = groups * states
    repeat = (iota((states, half), 1) % states == iota((states, half), 0)).astype(BF16)
    wide = jnp.dot(ref[...], repeat, preferred_element_type=F32)
    group = iota(wide.shape, 0) % width // (width // groups)
    wide = jnp.where(group == iota(wide.shape, 1) // states, wide, 0.0)
    return wide[:width], wide[width:]


def scan_part(x_ref, log_ref, loss_ref, eig_ref, freq_ref, win_ref, feed_ref,
              p_re, p_im, h_re, h_im, through_ref, a_re, a_im, d_re, d_im):
    _, positions = x_ref.shape
    groups, states = eig_ref.shape
    lanes = 128
    per = lanes // states
    x = x_ref[...].astype(F32).T
    through_ref[...] = x * feed_ref[...]
    steps = jnp.concatenate([jnp.exp(log_ref[...]), loss_ref[...]], axis=0).T
    eig, freq = flat(eig_ref), flat(freq_ref)
    x = x.astype(BF16)
    driven = [
        jnp.dot(x, w.astype(BF16), preferred_element_type=F32)
        for w in block_diagonal(win_ref, groups)
    ]
    half = groups * states
    for tile in range(half // lanes):
        at = slice(tile * lanes, (tile + 1) * lanes)
        place = iota((positions, lanes), 1) // states
        step = jnp.broadcast_to(steps[:, tile * per : tile * per + 1], (positions, lanes))
        loss = jnp.broadcast_to(
            steps[:, groups + tile * per : groups + tile * per + 1], (positions, lanes)
        )
        for k in range(1, per):
            g = tile * per + k
            step = jnp.where(place == k, steps[:, g : g + 1], step)
            loss = jnp.where(place == k, steps[:, groups + g : groups + g + 1], loss)
        decay_log = -eig[:, at] * step
        magnitude = jnp.exp(decay_log + loss)
        sin_x, cos_x = sin_cos(freq[:, at] * step)
        scaling = jnp.sqrt(minus_expm1(2.0 * decay_log))
        a_re[tile] = magnitude * cos_x
        a_im[tile] = magnitude * sin_x
        d_re[tile] = scaling * driven[0][:, at]
        d_im[tile] = scaling * driven[1][:, at]
    length = positions // CHUNKS
    ends = []
    for tile in range(half // lanes):
        at = slice(tile * lanes, (tile + 1) * lanes)
        for j in range(length):
            take = pl.ds(j, CHUNKS, stride=length)
            ar, ai = a_re[tile, take, :], a_im[tile, take, :]
            dr, di = d_re[tile, take, :], d_im[tile, take, :]
            if j == 0:
                pr, pi, hr, hi = ar, ai, dr, di
            else:
                pr, pi = pr * ar - pi * ai, pr * ai + pi * ar
                hr, hi = ar * hr - ai * hi + dr, ar * hi + ai * hr + di
            p_re[j, :, at], p_im[j, :, at] = pr, pi
            h_re[j, :, at], h_im[j, :, at] = hr, hi
        er, ei, sr, si = pr[0:1], pi[0:1], hr[0:1], hi[0:1]
        for c in range(1, CHUNKS):
            ar, ai = pr[c : c + 1], pi[c : c + 1]
            er, ei = er * ar - ei * ai, er * ai + ei * ar
            sr, si = ar * sr - ai * si + hr[c : c + 1], ar * si + ai * sr + hi[c : c + 1]
        ends += [er, ei, sr, si]
    ends = jnp.concatenate(ends, axis=0)
    high = ends.astype(BF16)
    return jnp.concatenate([high, (ends - high.astype(F32)).astype(BF16)], axis=1)


def readout_part(p_re, p_im, h_re, h_im, ends_ref, through_ref, wout_ref, turned):
    length, chunks, half = p_re.shape
    positions, width = through_ref.shape
    index = lax.axis_index("ep")
    cr = ci = jnp.zeros((1, half), F32)
    for b in range(ends_ref.shape[0] - 1):
        end = ends_ref[b, :, ends_ref.shape[2] - 256 :].astype(F32)
        end = end[:, :128] + end[:, 128:]
        ar, ai, er, ei = (
            jnp.concatenate([end[q : q + 1], end[q + 4 : q + 5]], axis=1) for q in range(4)
        )
        nr = ar * cr - ai * ci + er
        ni = ar * ci + ai * cr + ei
        keep = b < index
        cr, ci = jnp.where(keep, nr, cr), jnp.where(keep, ni, ci)
    carry_r, carry_i = [cr], [ci]
    for c in range(chunks - 1):
        ar, ai = p_re[length - 1, c : c + 1, :], p_im[length - 1, c : c + 1, :]
        cr, ci = (
            ar * cr - ai * ci + h_re[length - 1, c : c + 1, :],
            ar * ci + ai * cr + h_im[length - 1, c : c + 1, :],
        )
        carry_r.append(cr)
        carry_i.append(ci)
    cr = jnp.concatenate(carry_r, axis=0)[None]
    ci = jnp.concatenate(carry_i, axis=0)[None]
    sr = (h_re[...] + p_re[...] * cr - p_im[...] * ci).reshape(positions, half)
    si = (h_im[...] + p_re[...] * ci + p_im[...] * cr).reshape(positions, half)
    wr, wi = block_diagonal(wout_ref, half // wout_ref.shape[1])
    wr, wi = wr.astype(BF16), (-wi).astype(BF16)
    nothing = jnp.zeros((128 - width, half), BF16)
    wr, wi = (jnp.concatenate([w, nothing], axis=0) for w in (wr, wi))
    total = None
    for state, w in ((sr, wr), (si, wi)):
        high = state.astype(BF16)
        low = (state - high.astype(F32)).astype(BF16)
        for part in (high, low):
            got = lax.dot_general(part, w, NT, preferred_element_type=F32)
            total = got if total is None else total + got
    for j in range(length):
        turned[pl.ds(j, chunks, stride=length), :] = total[j * chunks : (j + 1) * chunks]
    v = turned[:, :width] + through_ref[...]
    v = 0.5 * v * (1.0 + jnp.tanh(0.7978845608028654 * (v + 0.044715 * (v * v * v))))
    both = positions // 2
    return jnp.concatenate([v[:both], v[both:]], axis=1).astype(BF16)


def block_of(ref, member, part):
    rows = ref.shape[1] // 2
    lanes = 128
    return jnp.concatenate(
        [
            ref[member, part * rows : (part + 1) * rows, i * lanes : (i + 1) * lanes]
            for i in range(ref.shape[2] // lanes)
        ],
        axis=0,
    )


def third_kernel(*refs):
    pieces, (scale_ref, w_ref, down_ref, mixed_ref, shared_ref, gains) = refs[:4], refs[4:]
    for d in range(gains.shape[0]):
        part = scale_ref[:, d * gains.shape[1] : (d + 1) * gains.shape[1]]
        gains[d : d + 1, :] = part
    sub = own_sub()
    members = pieces[0].shape[0]
    places = [(m, q) for m in range(members) for q in range(4)]
    blocks = [block_of(pieces[q], m, 0) for m, q in places]
    both, lanes = blocks[0].shape
    width = lanes // 2
    total = None
    for v in blocks:
        v = v.astype(F32)
        total = v * v if total is None else total + v * v
    first = iota((both, lanes), 1) < width
    count = 1.0 / (len(places) * width)
    sums = [jnp.sum(jnp.where(m, total, 0.0), axis=1, keepdims=True) for m in (first, ~first)]
    f0, f1 = (lax.rsqrt(s * count + EPS) for s in sums)
    factor = jnp.where(first, f0, f1)
    acc = [jnp.zeros((both, w_ref.shape[1]), F32)] * 2
    shared = jnp.zeros(shared_ref.shape, F32)
    for (m, q), block in zip(places, blocks):
        d = m * 4 + (sub ^ q ^ flipped(m))
        gain = jnp.concatenate([gains[pl.ds(d, 1), :]] * 2, axis=1)
        v = (block.astype(F32) * factor * gain).astype(BF16)
        w = w_ref[pl.ds(pl.multiple_of(d * width, width), width), :]
        w2 = jnp.concatenate([w, w], axis=0)
        for k, half in enumerate((first, ~first)):
            part = jnp.where(half, v, jnp.zeros_like(v))
            acc[k] = acc[k] + jnp.dot(part, w2, preferred_element_type=F32)
        shared = shared + jnp.dot(
            block_of(pieces[q], m, 1),
            down_ref[pl.ds(pl.multiple_of(d * lanes, lanes), lanes), :],
            preferred_element_type=F32,
        )
    mixed_ref[:both, :] = acc[0].astype(BF16)
    mixed_ref[both:, :] = acc[1].astype(BF16)
    shared_ref[...] = shared


def run_third(pieces, scale, w, down, positions, tokens):
    lanes = w.shape[1]
    return pl.pallas_call(
        third_kernel,
        out_shape=[
            jax.ShapeDtypeStruct((positions, lanes), BF16),
            jax.ShapeDtypeStruct((tokens, lanes), F32),
        ],
        in_specs=vmem(7),
        out_specs=vmem(2),
        scratch_shapes=[VM((pieces[0].shape[0] * 4, scale.size // pieces[0].shape[0] // 4), F32)],
        name="third",
    )(pieces[0], *held(*pieces[1:]), scale.reshape(1, -1), w, down)


def expert_table(routes_ref, weights_ref, experts):
    top, tokens = routes_ref.shape
    expert = iota((experts, tokens), 0)
    named = jnp.zeros((experts, tokens), F32)
    gain = jnp.zeros((experts, tokens), F32)
    for k in range(top):
        hit = routes_ref[k : k + 1, :] == expert
        named = jnp.where(hit, 1.0, named)
        if weights_ref is not None:
            gain = jnp.where(hit, weights_ref[k : k + 1, :], gain)
    earlier = (iota((tokens, tokens), 0) < iota((tokens, tokens), 1)).astype(BF16)
    rank = jnp.dot(named.astype(BF16), earlier, preferred_element_type=F32)
    return jnp.where(named > 0.0, rank, -1.0), gain


def own_place():
    return 2 * lax.axis_index("yl") + lax.axis_index("co")


def flipped(quad):
    return quad // 2 * 2


def own_sub():
    return own_place() ^ flipped(lax.axis_index("yh"))


def first_kernel(tokens_ref, gain_ref, routes_ref, *refs):
    scan_in, (normed_ref, sent_ref), scan_out = refs[:7], refs[7:9], refs[9:]
    ends = scan_part(*scan_in, *scan_out)
    tokens, width = tokens_ref.shape
    v = tokens_ref[...].astype(F32)
    factor = lax.rsqrt(jnp.mean(v * v, axis=1, keepdims=True) + EPS)
    normed = (v * factor * gain_ref[...]).astype(BF16)
    normed_ref[...] = normed
    share = ends.shape[0]
    experts = sent_ref.shape[0] // share
    rank, _ = expert_table(routes_ref, None, experts)
    slot = (iota((share, tokens), 0) + own_sub() * share).astype(F32)
    chosen = jnp.concatenate(
        [jnp.where(rank[e : e + 1, :] == slot, 1.0, 0.0) for e in range(experts)], axis=0
    ).astype(BF16)
    sent_ref[:, :width] = jnp.dot(chosen, normed, preferred_element_type=F32).astype(BF16)
    for e in range(experts):
        sent_ref[e * share : (e + 1) * share, width:] = ends


def run_first(tokens, gain, routes, blocks, x, log_step, loss, eig, freq, win, feed):
    width, positions = x.shape
    half = eig.size
    piece = jax.ShapeDtypeStruct((positions // CHUNKS, CHUNKS, half), F32)
    return pl.pallas_call(
        first_kernel,
        out_shape=[
            jax.ShapeDtypeStruct(tokens.shape, BF16),
            jax.ShapeDtypeStruct((blocks * half // 32, tokens.shape[1] + 256), BF16),
        ]
        + [piece] * 4
        + [jax.ShapeDtypeStruct((positions, width), F32)],
        in_specs=vmem(10),
        out_specs=vmem(7),
        scratch_shapes=[VM((half // 128, positions, 128), F32)] * 4,
        name="first",
    )(tokens, gain.reshape(1, -1), routes, x, log_step, loss, eig, freq, win, feed)


def choice_kernel(routes_ref, weights_ref, high_ref, low_ref):
    tokens = routes_ref.shape[1]
    share, parts = 8, 4
    experts = high_ref.shape[1] // (share * parts)
    rank, gain = expert_table(routes_ref, weights_ref, experts)
    for a in range(parts):
        held_by = a ^ flipped(lax.axis_index("yh"))
        slot = (iota((share, tokens), 0) + held_by * share).astype(F32)
        picked = jnp.concatenate(
            [
                jnp.where(rank[e : e + 1, :] == slot, gain[e : e + 1, :], 0.0)
                for e in range(experts)
            ],
            axis=0,
        ).T
        high = picked.astype(BF16)
        at = slice(a * experts * share, (a + 1) * experts * share)
        high_ref[:, at] = high
        low_ref[:, at] = (picked - high.astype(F32)).astype(BF16)


def run_choice(routes, weights, slots):
    return pl.pallas_call(
        choice_kernel,
        out_shape=[jax.ShapeDtypeStruct((routes.shape[1], slots), BF16)] * 2,
        in_specs=vmem(2),
        out_specs=vmem(2),
        name="choice",
    )(routes, weights)


def gated(got):
    half = got.shape[1] // 2
    gate, up = got[:, :half], got[:, half:]
    return (gate / (1.0 + jnp.exp(-gate)) * up).astype(BF16)


def second_kernel(arrived_ref, extra_ref, *refs):
    gates, ups, readout_in, (out_ref, turned) = refs[:4], refs[4:8], refs[8:14], refs[14:]
    mix = readout_part(*readout_in[:4], arrived_ref, *readout_in[4:], turned)
    blocks, share, _ = arrived_ref.shape
    rows = arrived_ref[:, :, : gates[0].shape[0]].reshape(blocks * share, -1)
    copies, _, wide = out_ref.shape
    lanes = mix.shape[1]
    for q, (gate, up) in enumerate(zip(gates, ups)):
        both = jnp.concatenate([gate[...], up[...]], axis=1)
        got = gated(jnp.dot(rows, both, preferred_element_type=F32))
        for copy in range(copies):
            out_ref[copy, : blocks * share, q * lanes : (q + 1) * lanes] = got
    at = blocks * share
    for item in (mix, extra_ref[...]):
        part = item.shape[0] * lanes // wide
        for i in range(wide // lanes):
            for copy in range(copies):
                out_ref[copy, at : at + part, i * lanes : (i + 1) * lanes] = item[
                    i * part : (i + 1) * part
                ]
        at += part


def run_second(arrived, extra, gates, ups, pieces, through, wout, copies):
    blocks, share, _ = arrived.shape
    wide = 4 * gates[0].shape[1]
    rows = blocks * share + (through.size + extra.size) // wide
    return pl.pallas_call(
        second_kernel,
        out_shape=jax.ShapeDtypeStruct((copies, rows, wide), BF16),
        in_specs=vmem(16),
        out_specs=pl.BlockSpec(memory_space=VM),
        scratch_shapes=[VM((through.shape[0], 128), F32)],
        name="second",
    )(*held(arrived), extra, *gates, *ups, *pieces, through, wout)


def shared_hidden_kernel(rows_ref, gate_ref, up_ref, out_ref):
    both = jnp.concatenate([gate_ref[...], up_ref[...]], axis=1)
    got = gated(jnp.dot(rows_ref[...], both, preferred_element_type=F32))
    out_ref[...] = got


def run_shared_hidden(rows, gate, up):
    return pl.pallas_call(
        shared_hidden_kernel,
        out_shape=jax.ShapeDtypeStruct((rows.shape[0], gate.shape[1]), BF16),
        in_specs=vmem(3),
        out_specs=pl.BlockSpec(memory_space=VM),
        name="shared_hidden",
    )(rows, gate, up)


def down_kernel(*refs):
    hidden, weights, (out_ref, rest_ref, whole) = refs[0], refs[1:5], refs[5:]
    rest_ref[...] = hidden[:, whole.shape[0] :, :]
    sub = own_sub()
    lanes = weights[0].shape[1]
    for member in range(hidden.shape[0]):
        for q in range(4):
            at = pl.multiple_of((member * 4 + (sub ^ q ^ flipped(member))) * lanes, lanes)
            whole[:, pl.ds(at, lanes)] = hidden[member, : whole.shape[0], q * lanes : (q + 1) * lanes]
    rows = whole[...]
    for q in (0, 2):
        both = jnp.concatenate([weights[q][...], weights[q + 1][...]], axis=1)
        got = jnp.dot(rows, both, preferred_element_type=F32).astype(BF16)
        out_ref[own_place() ^ q] = got[:, :lanes]
        out_ref[own_place() ^ (q + 1)] = got[:, lanes:]


def run_down(hidden, weights, rows):
    lanes = weights[0].shape[1]
    return pl.pallas_call(
        down_kernel,
        out_shape=[
            jax.ShapeDtypeStruct((4, rows, lanes), BF16),
            jax.ShapeDtypeStruct(
                (hidden.shape[0], hidden.shape[1] - rows, hidden.shape[2]), BF16
            ),
        ],
        in_specs=vmem(5),
        out_specs=vmem(2),
        scratch_shapes=[VM((rows, weights[0].shape[0]), BF16)],
        name="down",
    )(*held(hidden), *weights)


def combine_kernel(shared_ref, back_ref, high_ref, low_ref, out_ref):
    back = back_ref[...]
    total = shared_ref[...]
    for part in (high_ref, low_ref):
        total = total + jnp.dot(part[...], back, preferred_element_type=F32)
    out_ref[...] = total.astype(BF16)


def run_combine(shared, back, high, low):
    return pl.pallas_call(
        combine_kernel,
        out_shape=jax.ShapeDtypeStruct(shared.shape, BF16),
        in_specs=vmem(4),
        out_specs=pl.BlockSpec(memory_space=VM),
        name="combine",
    )(shared, *held(back, high, low))


TP = ("yh", "yl", "co")
SWAP = [(0, 1), (1, 0)]
LINES = [[0, 2, 5, 7], [1, 3, 4, 6]]


def exchanged(piece):
    over = lax.ppermute(piece, "yl", SWAP)
    core = lax.ppermute(piece, "co", SWAP)
    both = lax.ppermute(over, "co", SWAP)
    return (piece, core, over, both)


def spread_out(pieces, axes, groups=None):
    return lax.all_to_all(
        pieces, axes, split_axis=0, concat_axis=0, axis_index_groups=groups, tiled=True
    )


def on_device(
    mixer_group_input,
    log_step_size,
    extra_log_decay,
    negated_eigen_real,
    frequency,
    group_input_matrices,
    group_output_matrices,
    channel_feedthrough,
    mixer_norm_scale,
    mixer_output_weight,
    second_micro_input,
    expert_norm_scale,
    routes,
    chosen_expert_weight,
    expert_gate_weight,
    expert_up_weight,
    expert_down_weight,
    shared_gate_weight,
    shared_up_weight,
    shared_down_weight,
):
    blocks = lax.axis_size("ep")
    routes = routes.T
    normed, sent, *pieces, through = run_first(
        second_micro_input,
        expert_norm_scale,
        routes,
        blocks,
        mixer_group_input.T,
        log_step_size,
        extra_log_decay,
        negated_eigen_real,
        frequency,
        group_input_matrices.swapaxes(2, 3).reshape(-1, frequency.shape[1]),
        channel_feedthrough.reshape(1, -1),
    )
    arrived = spread_out(sent.reshape(blocks, 8, -1), "ep")
    gates = exchanged(expert_gate_weight[0])
    ups = exchanged(expert_up_weight[0])
    downs = exchanged(expert_down_weight[0])
    shared_hidden = run_shared_hidden(normed, shared_gate_weight, shared_up_weight)
    high, low = run_choice(routes, chosen_expert_weight.T, blocks * 32)

    hidden = run_second(
        arrived,
        shared_hidden,
        gates,
        ups,
        pieces,
        through,
        group_output_matrices.reshape(-1, frequency.shape[1]),
        lax.axis_size("yh"),
    )
    hidden = spread_out(hidden, ("yh", "yl"), LINES)
    results, own = run_down(hidden, downs, blocks * 8)
    results = results.reshape(4 * blocks, 8, -1)
    back = spread_out(results, ("yl", "co", "ep")).reshape(blocks * 32, -1)

    core = lax.ppermute(own, "co", SWAP)
    over = lax.ppermute(own, "yl", SWAP)
    both = lax.ppermute(over, "co", SWAP)
    mixed, shared = run_third(
        (own, core, over, both),
        mixer_norm_scale,
        mixer_output_weight,
        shared_down_weight,
        through.shape[0],
        routes.shape[1],
    )
    return (mixed, run_combine(shared, back, high, low))


def solution(mesh):
    finer = Mesh(
        mesh.devices.reshape(mesh.shape["ep"], mesh.shape["tp"] // 4, 2, 2), ("ep", *TP)
    )
    return jax.shard_map(
        on_device,
        mesh=finer,
        in_specs=(
            P("ep", TP),
            P(TP, "ep"),
            P(TP, "ep"),
            P(TP, None),
            P(TP, None),
            P(None, TP, None, None),
            P(None, TP, None, None),
            P(TP),
            P(),
            P(None, TP),
            P("ep", None),
            P(),
            P("ep", None),
            P("ep", None),
            P("ep", None, TP),
            P("ep", None, TP),
            P("ep", None, TP),
            P(None, TP),
            P(None, TP),
            P(None, TP),
        ),
        out_specs=(P("ep", TP), P("ep", TP)),
        check_vma=False,
    )
```

```python
import jax
import jax.numpy as jnp
from jax import lax
from jax.experimental import pallas as pl
from jax.experimental.pallas import tpu as pltpu
from jax.sharding import Mesh
from jax.sharding import PartitionSpec as P


VM = pltpu.VMEM
F32, BF16 = jnp.float32, jnp.bfloat16
NT = (((1,), (1,)), ((), ()))
EPS = 1e-06
CHUNKS = 8


def iota(shape, dim):
    return lax.broadcasted_iota(jnp.int32, shape, dim)


def vmem(count):
    return [pl.BlockSpec(memory_space=VM)] * count


def held(*arrays):
    return [pltpu.with_memory_space_constraint(a, VM) for a in arrays]


def sin_cos(x):
    turns = jnp.floor(x * 0.6366197723675814 + 0.5)
    r = x - turns * 1.5703125
    r = r - turns * 4.837512969970703e-4
    r = r - turns * 7.54978995489188e-8
    q = turns.astype(jnp.int32)
    s = r * r
    sin_r = r + r * s * (-1.6666654611e-1 + s * (8.3321608736e-3 - s * 1.9515295891e-4))
    cos_r = 1.0 - 0.5 * s + s * s * (
        4.166664568298827e-2 + s * (-1.388731625493765e-3 + s * 2.443315711809948e-5)
    )
    odd = (q & 1) == 1
    a = jnp.where(odd, cos_r, sin_r)
    b = jnp.where(odd, sin_r, cos_r)
    sin_x = jnp.where((q & 2) == 2, -a, a)
    cos_x = jnp.where(((q + 1) & 2) == 2, -b, b)
    return sin_x, cos_x


def minus_expm1(y):
    small = 1.0 + y * (1.0 / 9.0)
    for n in (8, 7, 6, 5, 4, 3, 2):
        small = 1.0 + y * (1.0 / n) * small
    return jnp.where(y > -0.5, -y * small, 1.0 - jnp.exp(y))


def flat(ref):
    return jnp.concatenate([ref[g : g + 1, :] for g in range(ref.shape[0])], axis=1)


def block_diagonal(ref, groups):
    rows, states = ref.shape
    width = rows // 2
    half = groups * states
    repeat = (iota((states, half), 1) % states == iota((states, half), 0)).astype(BF16)
    wide = jnp.dot(ref[...], repeat, preferred_element_type=F32)
    group = iota(wide.shape, 0) % width // (width // groups)
    wide = jnp.where(group == iota(wide.shape, 1) // states, wide, 0.0)
    return wide[:width], wide[width:]


def scan_part(x_ref, log_ref, loss_ref, eig_ref, freq_ref, win_ref, feed_ref,
              p_re, p_im, h_re, h_im, through_ref, a_re, a_im, d_re, d_im):
    _, positions = x_ref.shape
    groups, states = eig_ref.shape
    lanes = 128
    per = lanes // states
    x = x_ref[...].astype(F32).T
    through_ref[...] = x * feed_ref[...]
    steps = jnp.concatenate([jnp.exp(log_ref[...]), loss_ref[...]], axis=0).T
    eig, freq = flat(eig_ref), flat(freq_ref)
    x = x.astype(BF16)
    driven = [
        jnp.dot(x, w.astype(BF16), preferred_element_type=F32)
        for w in block_diagonal(win_ref, groups)
    ]
    half = groups * states
    for tile in range(half // lanes):
        at = slice(tile * lanes, (tile + 1) * lanes)
        place = iota((positions, lanes), 1) // states
        step = jnp.broadcast_to(steps[:, tile * per : tile * per + 1], (positions, lanes))
        loss = jnp.broadcast_to(
            steps[:, groups + tile * per : groups + tile * per + 1], (positions, lanes)
        )
        for k in range(1, per):
            g = tile * per + k
            step = jnp.where(place == k, steps[:, g : g + 1], step)
            loss = jnp.where(place == k, steps[:, groups + g : groups + g + 1], loss)
        decay_log = -eig[:, at] * step
        magnitude = jnp.exp(decay_log + loss)
        sin_x, cos_x = sin_cos(freq[:, at] * step)
        scaling = jnp.sqrt(minus_expm1(2.0 * decay_log))
        a_re[tile] = magnitude * cos_x
        a_im[tile] = magnitude * sin_x
        d_re[tile] = scaling * driven[0][:, at]
        d_im[tile] = scaling * driven[1][:, at]
    length = positions // CHUNKS
    ends = []
    for tile in range(half // lanes):
        at = slice(tile * lanes, (tile + 1) * lanes)
        for j in range(length):
            take = pl.ds(j, CHUNKS, stride=length)
            ar, ai = a_re[tile, take, :], a_im[tile, take, :]
            dr, di = d_re[tile, take, :], d_im[tile, take, :]
            if j == 0:
                pr, pi, hr, hi = ar, ai, dr, di
            else:
                pr, pi = pr * ar - pi * ai, pr * ai + pi * ar
                hr, hi = ar * hr - ai * hi + dr, ar * hi + ai * hr + di
            p_re[j, :, at], p_im[j, :, at] = pr, pi
            h_re[j, :, at], h_im[j, :, at] = hr, hi
        er, ei, sr, si = pr[0:1], pi[0:1], hr[0:1], hi[0:1]
        for c in range(1, CHUNKS):
            ar, ai = pr[c : c + 1], pi[c : c + 1]
            er, ei = er * ar - ei * ai, er * ai + ei * ar
            sr, si = ar * sr - ai * si + hr[c : c + 1], ar * si + ai * sr + hi[c : c + 1]
        ends += [er, ei, sr, si]
    ends = jnp.concatenate(ends, axis=0)
    high = ends.astype(BF16)
    return jnp.concatenate([high, (ends - high.astype(F32)).astype(BF16)], axis=1)


def readout_part(p_re, p_im, h_re, h_im, ends_ref, through_ref, wout_ref, turned):
    length, chunks, half = p_re.shape
    positions, width = through_ref.shape
    index = lax.axis_index("ep")
    cr = ci = jnp.zeros((1, half), F32)
    for b in range(ends_ref.shape[0] - 1):
        end = ends_ref[b, :, ends_ref.shape[2] - 256 :].astype(F32)
        end = end[:, :128] + end[:, 128:]
        ar, ai, er, ei = (
            jnp.concatenate([end[q : q + 1], end[q + 4 : q + 5]], axis=1) for q in range(4)
        )
        nr = ar * cr - ai * ci + er
        ni = ar * ci + ai * cr + ei
        keep = b < index
        cr, ci = jnp.where(keep, nr, cr), jnp.where(keep, ni, ci)
    carry_r, carry_i = [cr], [ci]
    for c in range(chunks - 1):
        ar, ai = p_re[length - 1, c : c + 1, :], p_im[length - 1, c : c + 1, :]
        cr, ci = (
            ar * cr - ai * ci + h_re[length - 1, c : c + 1, :],
            ar * ci + ai * cr + h_im[length - 1, c : c + 1, :],
        )
        carry_r.append(cr)
        carry_i.append(ci)
    cr = jnp.concatenate(carry_r, axis=0)[None]
    ci = jnp.concatenate(carry_i, axis=0)[None]
    sr = (h_re[...] + p_re[...] * cr - p_im[...] * ci).reshape(positions, half)
    si = (h_im[...] + p_re[...] * ci + p_im[...] * cr).reshape(positions, half)
    wr, wi = block_diagonal(wout_ref, half // wout_ref.shape[1])
    wr, wi = wr.astype(BF16), (-wi).astype(BF16)
    nothing = jnp.zeros((128 - width, half), BF16)
    wr, wi = (jnp.concatenate([w, nothing], axis=0) for w in (wr, wi))
    total = None
    for state, w in ((sr, wr), (si, wi)):
        high = state.astype(BF16)
        low = (state - high.astype(F32)).astype(BF16)
        for part in (high, low):
            got = lax.dot_general(part, w, NT, preferred_element_type=F32)
            total = got if total is None else total + got
    for j in range(length):
        turned[pl.ds(j, chunks, stride=length), :] = total[j * chunks : (j + 1) * chunks]
    v = turned[:, :width] + through_ref[...]
    v = 0.5 * v * (1.0 + jnp.tanh(0.7978845608028654 * (v + 0.044715 * (v * v * v))))
    both = positions // 2
    return jnp.concatenate([v[:both], v[both:]], axis=1).astype(BF16)


def block_of(ref, member, part):
    rows = ref.shape[1] // 2
    lanes = 128
    return jnp.concatenate(
        [
            ref[member, part * rows : (part + 1) * rows, i * lanes : (i + 1) * lanes]
            for i in range(ref.shape[2] // lanes)
        ],
        axis=0,
    )


def third_kernel(*refs):
    pieces, (scale_ref, w_ref, down_ref, mixed_ref, shared_ref, gains) = refs[:4], refs[4:]
    for d in range(gains.shape[0]):
        part = scale_ref[:, d * gains.shape[1] : (d + 1) * gains.shape[1]]
        gains[d : d + 1, :] = part
    sub = own_sub()
    members = pieces[0].shape[0]
    places = [(m, q) for m in range(members) for q in range(4)]
    blocks = [block_of(pieces[q], m, 0) for m, q in places]
    both, lanes = blocks[0].shape
    width = lanes // 2
    total = None
    for v in blocks:
        v = v.astype(F32)
        total = v * v if total is None else total + v * v
    first = iota((both, lanes), 1) < width
    count = 1.0 / (len(places) * width)
    sums = [jnp.sum(jnp.where(m, total, 0.0), axis=1, keepdims=True) for m in (first, ~first)]
    f0, f1 = (lax.rsqrt(s * count + EPS) for s in sums)
    factor = jnp.where(first, f0, f1)
    acc = [jnp.zeros((both, w_ref.shape[1]), F32)] * 2
    shared = jnp.zeros(shared_ref.shape, F32)
    for (m, q), block in zip(places, blocks):
        d = m * 4 + (sub ^ q ^ flipped(m))
        gain = jnp.concatenate([gains[pl.ds(d, 1), :]] * 2, axis=1)
        v = (block.astype(F32) * factor * gain).astype(BF16)
        w = w_ref[pl.ds(pl.multiple_of(d * width, width), width), :]
        w2 = jnp.concatenate([w, w], axis=0)
        for k, half in enumerate((first, ~first)):
            part = jnp.where(half, v, jnp.zeros_like(v))
            acc[k] = acc[k] + jnp.dot(part, w2, preferred_element_type=F32)
        shared = shared + jnp.dot(
            block_of(pieces[q], m, 1),
            down_ref[pl.ds(pl.multiple_of(d * lanes, lanes), lanes), :],
            preferred_element_type=F32,
        )
    mixed_ref[:both, :] = acc[0].astype(BF16)
    mixed_ref[both:, :] = acc[1].astype(BF16)
    shared_ref[...] = shared


def run_third(pieces, scale, w, down, positions, tokens):
    lanes = w.shape[1]
    return pl.pallas_call(
        third_kernel,
        out_shape=[
            jax.ShapeDtypeStruct((positions, lanes), BF16),
            jax.ShapeDtypeStruct((tokens, lanes), F32),
        ],
        in_specs=vmem(7),
        out_specs=vmem(2),
        scratch_shapes=[VM((pieces[0].shape[0] * 4, scale.size // pieces[0].shape[0] // 4), F32)],
        name="third",
    )(pieces[0], *held(*pieces[1:]), scale.reshape(1, -1), w, down)


def expert_table(routes_ref, weights_ref, experts):
    top, tokens = routes_ref.shape
    expert = iota((experts, tokens), 0)
    named = jnp.zeros((experts, tokens), F32)
    gain = jnp.zeros((experts, tokens), F32)
    for k in range(top):
        hit = routes_ref[k : k + 1, :] == expert
        named = jnp.where(hit, 1.0, named)
        if weights_ref is not None:
            gain = jnp.where(hit, weights_ref[k : k + 1, :], gain)
    earlier = (iota((tokens, tokens), 0) < iota((tokens, tokens), 1)).astype(BF16)
    rank = jnp.dot(named.astype(BF16), earlier, preferred_element_type=F32)
    return jnp.where(named > 0.0, rank, -1.0), gain


def own_place():
    return 2 * lax.axis_index("yl") + lax.axis_index("co")


def flipped(quad):
    return quad // 2 * 2


def own_sub():
    return own_place() ^ flipped(lax.axis_index("yh"))


def normed_rows(tokens_ref, gain_ref):
    v = tokens_ref[...].astype(F32)
    factor = lax.rsqrt(jnp.mean(v * v, axis=1, keepdims=True) + EPS)
    return (v * factor * gain_ref[...]).astype(BF16)


def first_kernel(tokens_ref, gain_ref, routes_ref, *refs):
    scan_in, sent_ref, scan_out = refs[:7], refs[7], refs[8:]
    tokens, width = tokens_ref.shape
    normed = normed_rows(tokens_ref, gain_ref)
    share = 8
    experts = sent_ref.shape[0] // share
    rank, _ = expert_table(routes_ref, None, experts)
    slot = (iota((share, tokens), 0) + own_sub() * share).astype(F32)
    chosen = jnp.concatenate(
        [jnp.where(rank[e : e + 1, :] == slot, 1.0, 0.0) for e in range(experts)], axis=0
    ).astype(BF16)
    sent_ref[:, :width] = jnp.dot(chosen, normed, preferred_element_type=F32).astype(BF16)
    ends = scan_part(*scan_in, *scan_out)
    for e in range(experts):
        sent_ref[e * share : (e + 1) * share, width:] = ends


def run_first(tokens, gain, routes, blocks, x, log_step, loss, eig, freq, win, feed):
    width, positions = x.shape
    half = eig.size
    piece = VM((positions // CHUNKS, CHUNKS, half), F32)
    return pl.pallas_call(
        first_kernel,
        out_shape=[
            jax.ShapeDtypeStruct((blocks * half // 32, tokens.shape[1] + 256), BF16),
        ]
        + [piece] * 4
        + [jax.ShapeDtypeStruct((positions, width), F32)],
        in_specs=vmem(10),
        out_specs=vmem(6),
        scratch_shapes=[VM((half // 128, positions, 128), F32)] * 4,
        name="first",
    )(tokens, gain.reshape(1, -1), routes, x, log_step, loss, eig, freq, win, feed)


def choice_kernel(routes_ref, weights_ref, high_ref, low_ref):
    tokens = routes_ref.shape[1]
    share, parts = 8, 4
    experts = high_ref.shape[1] // (share * parts)
    rank, gain = expert_table(routes_ref, weights_ref, experts)
    for a in range(parts):
        held_by = a ^ flipped(lax.axis_index("yh"))
        slot = (iota((share, tokens), 0) + held_by * share).astype(F32)
        picked = jnp.concatenate(
            [
                jnp.where(rank[e : e + 1, :] == slot, gain[e : e + 1, :], 0.0)
                for e in range(experts)
            ],
            axis=0,
        ).T
        high = picked.astype(BF16)
        at = slice(a * experts * share, (a + 1) * experts * share)
        high_ref[:, at] = high
        low_ref[:, at] = (picked - high.astype(F32)).astype(BF16)


def run_choice(routes, weights, slots):
    return pl.pallas_call(
        choice_kernel,
        out_shape=[jax.ShapeDtypeStruct((routes.shape[1], slots), BF16)] * 2,
        in_specs=vmem(2),
        out_specs=vmem(2),
        name="choice",
    )(routes, weights)


def gated(got):
    half = got.shape[1] // 2
    gate, up = got[:, :half], got[:, half:]
    return (gate / (1.0 + jnp.exp(-gate)) * up).astype(BF16)


def second_kernel(arrived_ref, extra_ref, *refs):
    gates, ups, readout_in, (out_ref, turned) = refs[:4], refs[4:8], refs[8:14], refs[14:]
    mix = readout_part(*readout_in[:4], arrived_ref, *readout_in[4:], turned)
    blocks, share, _ = arrived_ref.shape
    rows = arrived_ref[:, :, : gates[0].shape[0]].reshape(blocks * share, -1)
    copies, _, wide = out_ref.shape
    lanes = mix.shape[1]
    for q, (gate, up) in enumerate(zip(gates, ups)):
        both = jnp.concatenate([gate[...], up[...]], axis=1)
        got = gated(jnp.dot(rows, both, preferred_element_type=F32))
        for copy in range(copies):
            out_ref[copy, : blocks * share, q * lanes : (q + 1) * lanes] = got
    at = blocks * share
    for item in (mix, extra_ref[...]):
        part = item.shape[0] * lanes // wide
        for i in range(wide // lanes):
            for copy in range(copies):
                out_ref[copy, at : at + part, i * lanes : (i + 1) * lanes] = item[
                    i * part : (i + 1) * part
                ]
        at += part


def run_second(arrived, extra, gates, ups, pieces, through, wout, copies):
    blocks, share, _ = arrived.shape
    wide = 4 * gates[0].shape[1]
    rows = blocks * share + (through.size + extra.size) // wide
    return pl.pallas_call(
        second_kernel,
        out_shape=jax.ShapeDtypeStruct((copies, rows, wide), BF16),
        in_specs=vmem(16),
        out_specs=pl.BlockSpec(memory_space=VM),
        scratch_shapes=[VM((through.shape[0], 128), F32)],
        name="second",
    )(*held(arrived), extra, *gates, *ups, *held(*pieces), through, wout)


def shared_hidden_kernel(tokens_ref, gain_ref, gate_ref, up_ref, out_ref):
    rows = normed_rows(tokens_ref, gain_ref)
    both = jnp.concatenate([gate_ref[...], up_ref[...]], axis=1)
    got = gated(jnp.dot(rows, both, preferred_element_type=F32))
    out_ref[...] = got


def run_shared_hidden(tokens, gain, gate, up):
    return pl.pallas_call(
        shared_hidden_kernel,
        out_shape=jax.ShapeDtypeStruct((tokens.shape[0], gate.shape[1]), BF16),
        in_specs=vmem(4),
        out_specs=pl.BlockSpec(memory_space=VM),
        name="shared_hidden",
    )(tokens, gain.reshape(1, -1), gate, up)


def down_kernel(*refs):
    hidden, weights, (out_ref, rest_ref, whole) = refs[0], refs[1:5], refs[5:]
    rest_ref[...] = hidden[:, whole.shape[0] :, :]
    sub = own_sub()
    lanes = weights[0].shape[1]
    for member in range(hidden.shape[0]):
        for q in range(4):
            at = pl.multiple_of((member * 4 + (sub ^ q ^ flipped(member))) * lanes, lanes)
            whole[:, pl.ds(at, lanes)] = hidden[member, : whole.shape[0], q * lanes : (q + 1) * lanes]
    rows = whole[...]
    for q in (0, 2):
        both = jnp.concatenate([weights[q][...], weights[q + 1][...]], axis=1)
        got = jnp.dot(rows, both, preferred_element_type=F32).astype(BF16)
        out_ref[own_place() ^ q] = got[:, :lanes]
        out_ref[own_place() ^ (q + 1)] = got[:, lanes:]


def run_down(hidden, weights, rows):
    lanes = weights[0].shape[1]
    return pl.pallas_call(
        down_kernel,
        out_shape=[
            jax.ShapeDtypeStruct((4, rows, lanes), BF16),
            jax.ShapeDtypeStruct(
                (hidden.shape[0], hidden.shape[1] - rows, hidden.shape[2]), BF16
            ),
        ],
        in_specs=vmem(5),
        out_specs=vmem(2),
        scratch_shapes=[VM((rows, weights[0].shape[0]), BF16)],
        name="down",
    )(*held(hidden), *weights)


def combine_kernel(shared_ref, back_ref, high_ref, low_ref, out_ref):
    back = back_ref[...]
    total = shared_ref[...]
    for part in (high_ref, low_ref):
        total = total + jnp.dot(part[...], back, preferred_element_type=F32)
    out_ref[...] = total.astype(BF16)


def run_combine(shared, back, high, low):
    return pl.pallas_call(
        combine_kernel,
        out_shape=jax.ShapeDtypeStruct(shared.shape, BF16),
        in_specs=vmem(4),
        out_specs=pl.BlockSpec(memory_space=VM),
        name="combine",
    )(shared, *held(back, high, low))


TP = ("yh", "yl", "co")
SWAP = [(0, 1), (1, 0)]
LINES = [[0, 2, 5, 7], [1, 3, 4, 6]]


def exchanged(piece):
    over = lax.ppermute(piece, "yl", SWAP)
    core = lax.ppermute(piece, "co", SWAP)
    both = lax.ppermute(over, "co", SWAP)
    return (piece, core, over, both)


def spread_out(pieces, axes, groups=None):
    return lax.all_to_all(
        pieces, axes, split_axis=0, concat_axis=0, axis_index_groups=groups, tiled=True
    )


def on_device(
    mixer_group_input,
    log_step_size,
    extra_log_decay,
    negated_eigen_real,
    frequency,
    group_input_matrices,
    group_output_matrices,
    channel_feedthrough,
    mixer_norm_scale,
    mixer_output_weight,
    second_micro_input,
    expert_norm_scale,
    routes,
    chosen_expert_weight,
    expert_gate_weight,
    expert_up_weight,
    expert_down_weight,
    shared_gate_weight,
    shared_up_weight,
    shared_down_weight,
):
    blocks = lax.axis_size("ep")
    routes = routes.T
    sent, *pieces, through = run_first(
        second_micro_input,
        expert_norm_scale,
        routes,
        blocks,
        mixer_group_input.T,
        log_step_size,
        extra_log_decay,
        negated_eigen_real,
        frequency,
        group_input_matrices.swapaxes(2, 3).reshape(-1, frequency.shape[1]),
        channel_feedthrough.reshape(1, -1),
    )
    arrived = spread_out(sent.reshape(blocks, 8, -1), "ep")
    gates = exchanged(expert_gate_weight[0])
    ups = exchanged(expert_up_weight[0])
    downs = exchanged(expert_down_weight[0])
    shared_hidden = run_shared_hidden(
        second_micro_input, expert_norm_scale, shared_gate_weight, shared_up_weight
    )
    high, low = run_choice(routes, chosen_expert_weight.T, blocks * 32)

    hidden = run_second(
        arrived,
        shared_hidden,
        gates,
        ups,
        pieces,
        through,
        group_output_matrices.reshape(-1, frequency.shape[1]),
        lax.axis_size("yh"),
    )
    hidden = spread_out(hidden, ("yh", "yl"), LINES)
    results, own = run_down(hidden, downs, blocks * 8)
    results = results.reshape(4 * blocks, 8, -1)
    back = spread_out(results, ("yl", "co", "ep")).reshape(blocks * 32, -1)

    core = lax.ppermute(own, "co", SWAP)
    over = lax.ppermute(own, "yl", SWAP)
    both = lax.ppermute(over, "co", SWAP)
    mixed, shared = run_third(
        (own, core, over, both),
        mixer_norm_scale,
        mixer_output_weight,
        shared_down_weight,
        through.shape[0],
        routes.shape[1],
    )
    return (mixed, run_combine(shared, back, high, low))


def solution(mesh):
    finer = Mesh(
        mesh.devices.reshape(mesh.shape["ep"], mesh.shape["tp"] // 4, 2, 2), ("ep", *TP)
    )
    return jax.shard_map(
        on_device,
        mesh=finer,
        in_specs=(
            P("ep", TP),
            P(TP, "ep"),
            P(TP, "ep"),
            P(TP, None),
            P(TP, None),
            P(None, TP, None, None),
            P(None, TP, None, None),
            P(TP),
            P(),
            P(None, TP),
            P("ep", None),
            P(),
            P("ep", None),
            P("ep", None),
            P("ep", None, TP),
            P("ep", None, TP),
            P("ep", None, TP),
            P(None, TP),
            P(None, TP),
            P(None, TP),
        ),
        out_specs=(P("ep", TP), P("ep", TP)),
        check_vma=False,
    )
```
